128 devices in a mesh: sp: 16 (over z, y), tp: 8 (over x, core).
Axes of the slice: x: 4, y: 4, z: 4, core: 2. Of those that a mesh axis runs over, the one named last changes fastest.
Arguments:
- queries: bfloat16 [16384, 512], P('sp', 'tp'), may hold values from -6 to 6
- keys: bfloat16 [16384, 512], P('sp', 'tp'), may hold values from -6 to 6
- values: bfloat16 [16384, 1024], P('sp', 'tp'), may hold values from -6 to 6
- out_gate: bfloat16 [16384, 1024], P('sp', 'tp'), may hold values from -6 to 6
- decay_logit: float32 [2, 16384, 512], P(None, 'sp', 'tp'), may hold values from -8 to 16
- head_gain: float32 [1024], P('tp'), may hold values from 0.1 to 1.9
- out_weight: bfloat16 [1024, 2048], replicated, may hold values from -0.1875 to 0.1875
- stream: bfloat16 [16384, 2048], P(('sp', 'tp')), may hold values from -6 to 6
- mlp_gain: float32 [2048], replicated, may hold values from 0.1 to 1.9
- up_weight: bfloat16 [2048, 8192], P('sp', 'tp'), may hold values from -0.125 to 0.125
- down_weight: bfloat16 [8192, 2048], P('tp', 'sp'), may hold values from -0.0625 to 0.0625
Outputs:
- output: bfloat16 [16384, 2048], P(('sp', 'tp'))
The draws below stay inside these ranges and needn't reach their ends.
All inputs are finite; a program needn't handle non-finite values.
Results may differ from the reference program's by a relative error of at most 0.018.
Values may be sent and summed in bfloat16 or wider, within the bound.
No kernel may reach another device: no remote copies, remote signals or barrier semaphores. Data moves between devices by JAX's collectives and lax.ppermute only.
A program may use at most 128 MiB of HBM per device.

```python
import math
import jax
import jax.numpy as jnp
from jax import lax

D = 2048
HEADS = 8
HEAD_K = 64
HEAD_V = 128
FF = 8192
BLOCK = 64
TOK_DEV = 1024
SEQUENCE_TOKENS = 16384
KEY_W = 512
VALUE_W = 1024
N_TP = 8


def draw_decay_logit(key, part):
    partition_key = jax.random.split(key, 6)
    number_of_heads = KEY_W // HEAD_K
    shard_count = SEQUENCE_TOKENS // TOK_DEV
    fast_share = 0.5
    noise = 0.6 * jax.random.truncated_normal(partition_key[2], -3.0, 3.0, (2, SEQUENCE_TOKENS, number_of_heads, HEAD_K), jnp.float32)
    fast_heads = jax.random.bernoulli(partition_key[0], fast_share, (2, 1, number_of_heads, 1))
    shard_shift = jnp.repeat(jax.random.uniform(partition_key[1], (2, shard_count, 1, 1), jnp.float32, -0.7, 0.7), TOK_DEV, axis=1)
    channel_shift = jax.random.uniform(partition_key[3], (2, 1, number_of_heads, HEAD_K), jnp.float32, -1.0, 1.0)
    slow_level = math.log(SEQUENCE_TOKENS / 16.0) + 2.0 + shard_shift + channel_shift + noise
    fast_level = 1.0 + shard_shift + 0.5 * channel_shift + noise
    magnitude = jnp.where(fast_heads, fast_level, slow_level)
    spike_position = jax.random.randint(partition_key[4], (2, 4, 1), 0, SEQUENCE_TOKENS)
    token_positions = jnp.arange(SEQUENCE_TOKENS, dtype=jnp.int32)[None, None, :]
    spike_row_list = jnp.any(token_positions == spike_position, axis=1)
    spike_magnitude = jax.random.uniform(partition_key[5], (2, SEQUENCE_TOKENS, number_of_heads, 1), jnp.float32, -8.0, -4.0)
    magnitude = jnp.where(spike_row_list[:, :, None, None], spike_magnitude, magnitude)
    return magnitude.reshape(2, SEQUENCE_TOKENS, KEY_W).astype(jnp.float32)


def block_levels(key, shape, cuts, least, top_value):
    loudness = 1.0
    for axis_at, shards_of in cuts:
        heights = jax.random.uniform(jax.random.fold_in(jax.random.fold_in(key, 6), axis_at), (shards_of,), jnp.float32, least / len(cuts), top_value / len(cuts))
        loudness = loudness * jnp.repeat(jnp.exp(heights), shape[axis_at] // shards_of).reshape((-1,) + (1,) * (len(shape) - 1 - axis_at))
    return loudness


def normal_values(key, shape, width, bound, cuts=(), kind=jnp.bfloat16):
    gain = block_levels(key, shape, cuts, -0.22, 0.18) if cuts else 1.0
    result = jax.random.normal(key, shape, jnp.float32) * width * gain
    return jnp.minimum(jnp.maximum(result, -bound), bound).astype(kind)


def setup_inputs(seed: int = 0) -> dict:
    streams_of = jax.random.split(jax.random.key(seed), 12)
    queries = normal_values(streams_of[0], (SEQUENCE_TOKENS, KEY_W), 1.0, 6.0, ((0, 16), (1, 8)))
    keys = normal_values(streams_of[1], (SEQUENCE_TOKENS, KEY_W), 1.0, 6.0, ((0, 16), (1, 8)))
    values = normal_values(streams_of[2], (SEQUENCE_TOKENS, VALUE_W), 1.0, 6.0, ((0, 16), (1, 8)))
    out_gate = normal_values(streams_of[3], (SEQUENCE_TOKENS, VALUE_W), 1.0, 6.0, ((0, 16), (1, 8)))
    decay_logit = draw_decay_logit(jax.random.fold_in(streams_of[11], 71), 0)
    head_gain = jnp.clip(1.0 + 0.18 * jax.random.normal(streams_of[5], (VALUE_W,), jnp.float32), 0.1, 1.9)
    out_weight = normal_values(streams_of[6], (VALUE_W, D), VALUE_W ** -0.5, 0.1875)
    stream = normal_values(streams_of[7], (SEQUENCE_TOKENS, D), 1.0, 6.0, ((0, 128),))
    mlp_gain = jnp.clip(1.0 + 0.18 * jax.random.normal(streams_of[8], (D,), jnp.float32), 0.1, 1.9)
    up_weight = normal_values(streams_of[9], (D, FF), D ** -0.5, 0.125, ((0, 16), (1, 8)))
    down_weight = normal_values(streams_of[10], (FF, D), FF ** -0.5, 0.0625, ((0, 8), (1, 16)))
    return dict(queries=queries, keys=keys, values=values, out_gate=out_gate, decay_logit=decay_logit, head_gain=head_gain, out_weight=out_weight, stream=stream, mlp_gain=mlp_gain, up_weight=up_weight, down_weight=down_weight)


gate_temper = 16.0
norm_eps = 1e-06
highest = lax.Precision.HIGHEST

def blockwise(query_rows, key_rows, value_rows, log_decay):
    length, number_of_heads, key_size = query_rows.shape
    value_size = value_rows.shape[2]
    block_count = length // BLOCK
    query_blk = query_rows.reshape(block_count, BLOCK, number_of_heads, key_size)
    key_blk = key_rows.reshape(block_count, BLOCK, number_of_heads, key_size)
    value_blk = value_rows.reshape(block_count, BLOCK, number_of_heads, value_size)
    within = jnp.cumsum(log_decay.reshape(block_count, BLOCK, number_of_heads, key_size), axis=1)
    block_end = within[:, -1]
    query_dec = query_blk * jnp.exp(within)
    key_inv = key_blk * jnp.exp(-within)
    key_end = key_blk * jnp.exp(block_end[:, None] - within)
    lower_mask = jnp.tril(jnp.ones((BLOCK, BLOCK), dtype=bool))
    scores = jnp.einsum('nihd,njhd->nhij', query_dec, key_inv, precision=highest)
    scores = jnp.where(lower_mask, scores, jnp.float32(0.0))
    intra_out = jnp.einsum('nhij,njhe->nihe', scores, value_blk, precision=highest)
    increments = jnp.einsum('njhd,njhe->nhde', key_end, value_blk, precision=highest)

    def advance(carried, inputs):
        decay_end, increment = inputs
        return (decay_end[..., None] * carried + increment, carried)
    start_state = jnp.zeros((number_of_heads, key_size, value_size), jnp.float32)
    state_end, state_in = lax.scan(advance, start_state, (jnp.exp(block_end), increments))
    inter_out = jnp.einsum('nihd,nhde->nihe', query_dec, state_in, precision=highest)
    return ((intra_out + inter_out).reshape(length, number_of_heads, value_size), state_end)

def reference(queries, keys, values, out_gate, decay_logit, head_gain, out_weight, stream, mlp_gain, up_weight, down_weight):
    length = queries.shape[0]
    query_heads = queries.astype(jnp.float32).reshape(length, HEADS, HEAD_K) * HEAD_K ** (-0.5)
    key_heads = keys.astype(jnp.float32).reshape(length, HEADS, HEAD_K)
    value_heads = values.astype(jnp.float32).reshape(length, HEADS, HEAD_V)
    log_decay = (jax.nn.log_sigmoid(decay_logit) / gate_temper).reshape(2, length, HEADS, HEAD_K)
    forward_out = blockwise(query_heads, key_heads, value_heads, log_decay[0])[0]
    backward_out = blockwise(jnp.flip(query_heads, 0), jnp.flip(key_heads, 0), jnp.flip(value_heads, 0), jnp.flip(log_decay[1], 0))[0]
    attended = forward_out + jnp.flip(backward_out, 0)
    inv_rms = lax.rsqrt(lax.optimization_barrier(jnp.mean(attended * attended, axis=-1, keepdims=True)) + norm_eps)
    normed_heads = (attended * inv_rms * head_gain.reshape(HEADS, HEAD_V)).reshape(length, VALUE_W)
    gated = (normed_heads * jax.nn.silu(out_gate.astype(jnp.float32))).astype(jnp.bfloat16)
    residual = (stream.astype(jnp.float32) + jnp.dot(gated, out_weight, preferred_element_type=jnp.float32)).astype(jnp.bfloat16)
    group_width = FF // N_TP

    def feed_forward(block_rows):
        widened = block_rows.astype(jnp.float32)
        row_rms = lax.rsqrt(lax.optimization_barrier(jnp.mean(widened * widened, axis=-1, keepdims=True)) + norm_eps)
        normed = (widened * row_rms * mlp_gain).astype(jnp.bfloat16)
        hidden = jnp.square(jax.nn.relu(jnp.dot(normed, up_weight, preferred_element_type=jnp.float32))).astype(jnp.bfloat16)
        summed = jnp.zeros(widened.shape, jnp.float32)
        for group in range(N_TP):
            group_part = jnp.dot(hidden[:, group * group_width:(group + 1) * group_width], down_weight[group * group_width:(group + 1) * group_width], preferred_element_type=jnp.float32).astype(jnp.bfloat16)
            group_part = lax.optimization_barrier(group_part)
            summed = summed + group_part.astype(jnp.float32)
        return (widened + summed).astype(jnp.bfloat16)
    output = lax.map(feed_forward, residual.reshape(length // TOK_DEV, TOK_DEV, D))
    return output.reshape(length, D)
```

```python
import functools

import jax
import jax.numpy as jnp
from jax import lax
from jax.experimental import pallas as pl
from jax.experimental.pallas import tpu as pltpu
from jax.sharding import Mesh
from jax.sharding import PartitionSpec as P


HEAD_K = 64
HEAD_V = 128
BLOCK = 128
D = 2048
ROWS = 128
SP = ("z", "y")
TP = ("x", "c")
PEERS = 16
FOLD = 80

gate_temper = 16.0
norm_eps = 1e-06
f32 = jnp.float32
bf16 = jnp.bfloat16
NEAR = (0, -1, 1, 2)

VMEM = pl.BlockSpec(memory_space=pltpu.VMEM)
SMEM = pl.BlockSpec(memory_space=pltpu.SMEM)
ANY = pl.BlockSpec(memory_space=pl.ANY)


def dot(a, b, dims=((1,), (0,)), precision=None):
    return lax.dot_general(a, b, (dims, ((), ())), precision=precision, preferred_element_type=f32)


def attend_kernel(pos, q_ref, k_ref, v_ref, ld_ref, local_ref, carry_ref, send_ref, qd_s, tot_s, inc_s):
    length = q_ref.shape[0]
    count = length // BLOCK
    me = pos[0] * 4 + pos[1]
    row = lax.broadcasted_iota(jnp.int32, (BLOCK, BLOCK), 0)
    col = lax.broadcasted_iota(jnp.int32, (BLOCK, BLOCK), 1)
    ahead = col < HEAD_K
    lower = jnp.where(row >= col, 1.0, 0.0).astype(bf16)

    for b in range(count):
        rows = slice(b * BLOCK, (b + 1) * BLOCK)
        logit = jnp.concatenate([ld_ref[0, rows], ld_ref[1, rows]], axis=1)
        decay = (jnp.minimum(logit, 0.0) - jnp.log1p(jnp.exp(-jnp.abs(logit)))) / gate_temper
        high = decay.astype(bf16)
        low = (decay - high.astype(f32)).astype(bf16)
        run = dot(lower, high) + dot(lower, low)
        total = run[BLOCK - 1 : BLOCK]
        within = jnp.where(ahead, run, total - run + decay)
        grow = jnp.exp(-within)
        q2 = jnp.concatenate([q_ref[rows], q_ref[rows]], axis=1).astype(f32)
        k2 = jnp.concatenate([k_ref[rows], k_ref[rows]], axis=1).astype(f32)
        q_dec = q2 * (jnp.exp(within) * HEAD_K ** (-0.5))
        k_inv = k2 * grow
        k_end = (k2 * jnp.exp(total - within)).astype(bf16)
        k_low = k_inv.astype(bf16)
        v_blk = v_ref[rows]
        fwd = dot(jnp.where(ahead, q_dec, 0.0).astype(bf16), k_low, ((1,), (1,)))
        bwd = dot(jnp.where(ahead, 0.0, q_dec).astype(bf16), k_low, ((1,), (1,)))
        scores = jnp.where(row >= col, fwd, 0.0) + jnp.where(row <= col, bwd, 0.0)
        local_ref[rows] = dot(scores.astype(bf16), v_blk)
        inc_s[b] = dot(v_blk, k_end, ((0,), (0,)))
        qd_s[rows] = q_dec
        tot_s[b : b + 1] = total

    totals = [tot_s[b : b + 1] for b in range(count)]
    ends = [jnp.exp(t) for t in totals]
    ahead1 = ahead[:1]
    forward = [jnp.zeros((HEAD_V, 2 * HEAD_K), f32)]
    before = [jnp.zeros_like(totals[0])]
    for b in range(count):
        forward.append(forward[b] * ends[b] + inc_s[b])
        before.append(before[b] + totals[b])
    backward = [jnp.zeros((HEAD_V, 2 * HEAD_K), f32)]
    after = [jnp.zeros_like(totals[0])]
    for b in reversed(range(count)):
        backward.append(backward[-1] * ends[b] + inc_s[b])
        after.append(after[-1] + totals[b])
    for b in range(count):
        rows = slice(b * BLOCK, (b + 1) * BLOCK)
        state = jnp.where(ahead, forward[b], backward[count - 1 - b]).astype(bf16)
        q_dec = qd_s[rows]
        local_ref[rows] = local_ref[rows] + dot(q_dec.astype(bf16), state, ((1,), (1,)))
        reach = jnp.exp(jnp.where(ahead1, before[b], after[count - 1 - b]))
        carry_ref[rows] = (q_dec * reach).astype(bf16)

    whole = jnp.exp(before[count])
    half = HEAD_V // 2

    def folded(state, lanes):
        wide = jnp.concatenate([state[:half, lanes], state[half:, lanes]], axis=1)
        decay = jnp.concatenate([whole[:, lanes], whole[:, lanes]], axis=1)
        return wide.astype(bf16), jnp.broadcast_to(decay, (FOLD - half, 2 * HEAD_K)).astype(bf16)

    to_later = folded(forward[count], slice(0, HEAD_K))
    to_earlier = folded(backward[count], slice(HEAD_K, 2 * HEAD_K))
    for peer in range(PEERS):
        later = peer > me
        send_ref[peer, :half] = jnp.where(later, to_later[0], to_earlier[0])
        send_ref[peer, half:] = jnp.where(later, to_later[1], to_earlier[1])


def gate_kernel(pos, got_ref, local_ref, carry_ref, gate_ref, gain_ref, keep_ref, give_ref, both_s):
    me = pos[0] * 4 + pos[1]
    half = HEAD_V // 2
    fwd = jnp.zeros((half, 2 * HEAD_K), f32)
    bwd = jnp.zeros((half, 2 * HEAD_K), f32)
    for peer in range(PEERS):
        state = got_ref[peer, :half].astype(f32)
        decay = got_ref[peer, half : half + 16].astype(f32)[:1]
        fwd = jnp.where(peer < me, fwd * decay + state, fwd)
    for peer in reversed(range(PEERS)):
        state = got_ref[peer, :half].astype(f32)
        decay = got_ref[peer, half : half + 16].astype(f32)[:1]
        bwd = jnp.where(peer > me, bwd * decay + state, bwd)
    top = jnp.concatenate([fwd[:, :HEAD_K], bwd[:, :HEAD_K]], axis=1)
    low = jnp.concatenate([fwd[:, HEAD_K:], bwd[:, HEAD_K:]], axis=1)
    state = jnp.concatenate([top, low], axis=0).astype(bf16)
    for group in range(8):
        rows = slice(group * ROWS, (group + 1) * ROWS)
        out = local_ref[rows] + dot(carry_ref[rows], state, ((1,), (1,)))
        scale = lax.rsqrt(jnp.mean(out * out, axis=-1, keepdims=True) + norm_eps)
        gate = gate_ref[rows].astype(f32)
        gate = gate / (1.0 + jnp.exp(-gate))
        both_s[lax.bitwise_xor(pos[3], group % 2), group // 2] = (out * scale * gain_ref[...] * gate).astype(bf16)
    keep_ref[...] = both_s[0]
    give_ref[...] = both_s[1]


def mix_kernel(pos, g0, g1, g2, g3, s0, s1, s2, s3, w_ref, gain_ref, normed_ref, own_ref, xs, res):
    first = pos[3] == 0
    for d, g in enumerate((g0, g1, g2, g3)):
        for k in range(4):
            at = lax.rem(pos[2] + (NEAR[k] + 4), 4)
            a, b = g[0, at], g[1, at]
            xs[k * ROWS : (k + 1) * ROWS, d * 256 : d * 256 + 128] = jnp.where(first, a, b)
            xs[k * ROWS : (k + 1) * ROWS, d * 256 + 128 : (d + 1) * 256] = jnp.where(first, b, a)
    squares = jnp.zeros((4 * ROWS, 128), f32)
    wide = 512
    for n in range(D // wide):
        cols = slice(n * wide, (n + 1) * wide)
        acc = None
        for d in range(4):
            at = pl.multiple_of(lax.rem(pos[2] + (NEAR[d] + 4), 4) * 256, 256)
            part = dot(xs[:, d * 256 : (d + 1) * 256], w_ref[pl.ds(at, 256), cols])
            acc = part if acc is None else acc + part
        for k, s in enumerate((s0, s1, s2, s3)):
            rows = slice(k * ROWS, (k + 1) * ROWS)
            res[rows, cols] = (s[:, cols].astype(f32) + acc[rows]).astype(bf16)
        line = res[:, cols].astype(f32)
        line = line * line
        for j in range(wide // 128):
            squares = squares + line[:, j * 128 : (j + 1) * 128]
    scale = lax.rsqrt(jnp.sum(squares, axis=-1, keepdims=True) / D + norm_eps)
    for n in range(D // wide):
        cols = slice(n * wide, (n + 1) * wide)
        normed_ref[:, cols] = (res[:, cols].astype(f32) * scale * gain_ref[:, cols]).astype(bf16)
    own_ref[...] = res[:ROWS]


def placed(pos, first_axis):
    z, y = pos[0], pos[1]
    e = 2 * pos[3] - 1

    def spot(a, b):
        dz, dy = (b, a) if first_axis == "y" else (a, b)
        return lax.rem(z + dz + 8, 4) * 4 + lax.rem(y + dy + 8, 4)

    mine, other = (0, e, -e, 2), (0, -e, e, 2)
    out = []
    for i in range(8):
        out.append((0, i, spot(mine[i % 4], 0), i // 4))
    for i in range(8):
        out.append((1, i, spot(mine[i % 4], e), i // 4))
    for i in range(8):
        out.append((2, i, spot(other[i % 4], -e), 1 - i // 4))
    for i in range(4):
        out.append((3, i, spot(mine[i], 2), 0))
    for i in range(4):
        out.append((4, i, spot(other[i], 2), 1))
    return out


def ff_kernel(pos, x_ref, u0, u1, u2, u3, u4, d0, d1, d2, d3, d4, o0, o1, o2, o3, wu, wd, hid, sems):
    ups, downs = [], []
    for p, (a, i, sp, half) in enumerate(placed(pos, "y")):
        src = (u0, u1, u2, u3, u4)[a].at[i]
        dst = wu.at[pl.ds(pl.multiple_of(sp * 128, 128), 128), pl.ds(half * 1024, 1024)]
        ups.append(pltpu.make_async_copy(src, dst, sems.at[p]))
    for p, (a, i, sp, half) in enumerate(placed(pos, "z")):
        src = (d0, d1, d2, d3, d4)[a].at[i]
        dst = wd.at[pl.ds(half * 1024, 1024), pl.ds(pl.multiple_of(sp * 128, 128), 128)]
        downs.append(pltpu.make_async_copy(src, dst, sems.at[32 + p]))
    for copy in ups + downs:
        copy.start()
    for copy in ups:
        copy.wait()
    wide = 512

    @pl.loop(0, D // wide)
    def _(n):
        cols = pl.ds(pl.multiple_of(n * wide, wide), wide)
        h = jnp.maximum(dot(x_ref[...], wu[:, cols]), 0.0)
        hid[:, cols] = (h * h).astype(bf16)

    for copy in downs:
        copy.wait()

    @pl.loop(0, D // wide)
    def _(n):
        cols = pl.ds(pl.multiple_of(n * wide, wide), wide)
        part = dot(hid[...], wd[:, cols]).astype(bf16)
        for k, o in enumerate((o0, o1, o2, o3)):
            o[:, cols] = part[k * ROWS : (k + 1) * ROWS]


def call(kernel, ins, outs, scratch, args, flops, nbytes, limit=48):
    return pl.pallas_call(
        kernel,
        in_specs=ins,
        out_specs=[VMEM] * len(outs),
        out_shape=[jax.ShapeDtypeStruct(s, t) for s, t in outs],
        scratch_shapes=scratch,
        cost_estimate=pl.CostEstimate(flops=flops, bytes_accessed=nbytes, transcendentals=0),
        compiler_params=pltpu.CompilerParams(vmem_limit_bytes=limit * 1024 * 1024),
    )(*args)


def shifted(v, axis, by, n=4):
    return lax.ppermute(v, axis, [(i, (i + by) % n) for i in range(n)])


def swapped(v):
    return lax.ppermute(v, "c", [(0, 1), (1, 0)])


def both_ways(v, axis):
    pairs = [(2 * i + c, 2 * ((i + 1 - 2 * c) % 4) + c) for i in range(4) for c in range(2)]
    return lax.ppermute(v, (axis, "c"), pairs)


def gathered(w, first, second):
    own = jnp.stack([w, swapped(w)])
    near = both_ways(own, first)
    near_s = swapped(near)
    far = both_ways(near[0], first)
    far_s = swapped(far)
    line = jnp.stack([own[0], near[0], near_s[1], far, own[1], near[1], near_s[0], far_s])
    return line


def spread(line, axis):
    near = both_ways(line, axis)
    near_s = swapped(near)
    far = both_ways(near[:4], axis)
    far_s = swapped(far)
    return line, near, near_s, far, far_s


def local(
    queries,
    keys,
    values,
    out_gate,
    decay_logit,
    head_gain,
    out_weight,
    stream,
    mlp_gain,
    up_weight,
    down_weight,
):
    length = queries.shape[0]
    pos = jnp.stack([lax.axis_index(a) for a in ("z", "y", "x", "c")]).astype(jnp.int32)

    up_line = gathered(up_weight, "y", "z")
    down_line = gathered(down_weight, "z", "y")
    streams = [stream, shifted(stream, "x", 1), shifted(stream, "x", -1), shifted(stream, "x", 2)]

    rows_out, carry, sent = call(
        attend_kernel,
        [SMEM] + [VMEM] * 4,
        [((length, HEAD_V), f32), ((length, 2 * HEAD_K), bf16), ((PEERS, FOLD, 128), bf16)],
        [
            pltpu.VMEM((length, 2 * HEAD_K), f32),
            pltpu.VMEM((length // BLOCK, 2 * HEAD_K), f32),
            pltpu.VMEM((length // BLOCK, HEAD_V, 2 * HEAD_K), f32),
        ],
        (pos, queries, keys, values, decay_logit),
        2_000_000_000,
        2_000_000,
    )
    got = lax.all_to_all(sent, SP, 0, 0, tiled=True)
    up_line, down_line, got = lax.optimization_barrier((up_line, down_line, got))
    ups = spread(up_line, "z")
    downs = spread(down_line, "y")
    keep, give = call(
        gate_kernel,
        [SMEM] + [VMEM] * 5,
        [((4, ROWS, HEAD_V), bf16)] * 2,
        [pltpu.VMEM((2, 4, ROWS, HEAD_V), bf16)],
        (pos, got, rows_out, carry, out_gate, head_gain.reshape(1, HEAD_V)),
        1_000_000_000,
        2_000_000,
    )
    pair = jnp.stack([keep, swapped(give)])
    heads = [pair, shifted(pair, "x", 1), shifted(pair, "x", -1), shifted(pair, "x", 2)]
    normed, residual = call(
        mix_kernel,
        [SMEM] + [VMEM] * 10,
        [((4 * ROWS, D), bf16), ((ROWS, D), bf16)],
        [pltpu.VMEM((4 * ROWS, 1024), bf16), pltpu.VMEM((4 * ROWS, D), bf16)],
        (pos, *heads, *streams, out_weight, mlp_gain.reshape(1, D)),
        2 * 512 * 1024 * 2048,
        12_000_000,
    )
    parts = call(
        ff_kernel,
        [SMEM, VMEM] + [ANY] * 10,
        [((ROWS, D), bf16)] * 4,
        [
            pltpu.VMEM((D, 2048), bf16),
            pltpu.VMEM((2048, D), bf16),
            pltpu.VMEM((4 * ROWS, 2048), bf16),
            pltpu.SemaphoreType.DMA((64,)),
        ],
        (pos, normed, *ups, *downs),
        4 * 512 * 2048 * 2048,
        20_000_000,
    )
    back = [shifted(parts[k], "x", NEAR[k]) for k in (1, 2, 3)]
    total = parts[0].astype(f32) + back[0].astype(f32) + back[1].astype(f32) + back[2].astype(f32)
    return (residual.astype(f32) + total).astype(bf16)


def solution(mesh):
    split = Mesh(mesh.devices.reshape(4, 4, 4, 2), ("z", "y", "x", "c"))
    both = SP + TP
    in_specs = (
        P(SP, TP),
        P(SP, TP),
        P(SP, TP),
        P(SP, TP),
        P(None, SP, TP),
        P(TP),
        P(),
        P(both, None),
        P(),
        P(SP, TP),
        P(TP, SP),
    )
    return jax.shard_map(local, mesh=split, in_specs=in_specs, out_specs=P(both, None), check_vma=False)
```

```python
import functools

import jax
import jax.numpy as jnp
from jax import lax
from jax.experimental import pallas as pl
from jax.experimental.pallas import tpu as pltpu
from jax.sharding import Mesh
from jax.sharding import PartitionSpec as P


HEAD_K = 64
HEAD_V = 128
BLOCK = 128
D = 2048
ROWS = 128
SP = ("z", "y")
TP = ("x", "c")
PEERS = 16
FOLD = 80

gate_temper = 16.0
norm_eps = 1e-06
f32 = jnp.float32
bf16 = jnp.bfloat16
NEAR = (0, -1, 1, 2)

VMEM = pl.BlockSpec(memory_space=pltpu.VMEM)
SMEM = pl.BlockSpec(memory_space=pltpu.SMEM)
ANY = pl.BlockSpec(memory_space=pl.ANY)
HBM = pl.BlockSpec(memory_space=pltpu.HBM)


def dot(a, b, dims=((1,), (0,)), precision=None):
    return lax.dot_general(a, b, (dims, ((), ())), precision=precision, preferred_element_type=f32)


def attend_kernel(pos, q_ref, k_ref, v_ref, ld_ref, local_ref, carry_ref, send_ref, qd_s, tot_s, inc_s):
    length = q_ref.shape[1]
    count = length // BLOCK
    me = pos[0] * 4 + pos[1]
    row = lax.broadcasted_iota(jnp.int32, (BLOCK, BLOCK), 0)
    col = lax.broadcasted_iota(jnp.int32, (BLOCK, BLOCK), 1)
    ahead = col < HEAD_K
    lower = jnp.where(row >= col, 1.0, 0.0).astype(bf16)

    for b in range(count):
        rows = slice(b * BLOCK, (b + 1) * BLOCK)
        logit = jnp.concatenate([ld_ref[0, :, rows], ld_ref[1, :, rows]], axis=0).T
        decay = (jnp.minimum(logit, 0.0) - jnp.log1p(jnp.exp(-jnp.abs(logit)))) / gate_temper
        high = decay.astype(bf16)
        low = (decay - high.astype(f32)).astype(bf16)
        run = dot(lower, high) + dot(lower, low)
        total = run[BLOCK - 1 : BLOCK]
        within = jnp.where(ahead, run, total - run + decay)
        grow = jnp.exp(-within)
        q_blk, k_blk = q_ref[:, rows].astype(f32), k_ref[:, rows].astype(f32)
        q2 = jnp.concatenate([q_blk, q_blk], axis=0).T
        k2 = jnp.concatenate([k_blk, k_blk], axis=0).T
        q_dec = q2 * (jnp.exp(within) * HEAD_K ** (-0.5))
        k_inv = k2 * grow
        k_end = (k2 * jnp.exp(total - within)).astype(bf16)
        k_low = k_inv.astype(bf16)
        v_blk = v_ref[rows]
        fwd = dot(jnp.where(ahead, q_dec, 0.0).astype(bf16), k_low, ((1,), (1,)))
        bwd = dot(jnp.where(ahead, 0.0, q_dec).astype(bf16), k_low, ((1,), (1,)))
        scores = jnp.where(row >= col, fwd, 0.0) + jnp.where(row <= col, bwd, 0.0)
        local_ref[rows] = dot(scores.astype(bf16), v_blk)
        inc_s[b] = dot(v_blk, k_end, ((0,), (0,)))
        qd_s[rows] = q_dec
        tot_s[b : b + 1] = total

    totals = [tot_s[b : b + 1] for b in range(count)]
    ends = [jnp.exp(t) for t in totals]
    ahead1 = ahead[:1]
    forward = [jnp.zeros((HEAD_V, 2 * HEAD_K), f32)]
    before = [jnp.zeros_like(totals[0])]
    for b in range(count):
        forward.append(forward[b] * ends[b] + inc_s[b])
        before.append(before[b] + totals[b])
    backward = [jnp.zeros((HEAD_V, 2 * HEAD_K), f32)]
    after = [jnp.zeros_like(totals[0])]
    for b in reversed(range(count)):
        backward.append(backward[-1] * ends[b] + inc_s[b])
        after.append(after[-1] + totals[b])
    for b in range(count):
        rows = slice(b * BLOCK, (b + 1) * BLOCK)
        state = jnp.where(ahead, forward[b], backward[count - 1 - b]).astype(bf16)
        q_dec = qd_s[rows]
        local_ref[rows] = local_ref[rows] + dot(q_dec.astype(bf16), state, ((1,), (1,)))
        reach = jnp.exp(jnp.where(ahead1, before[b], after[count - 1 - b]))
        carry_ref[rows] = (q_dec * reach).astype(bf16)

    whole = jnp.exp(before[count])
    half = HEAD_V // 2

    def folded(state, lanes):
        wide = jnp.concatenate([state[:half, lanes], state[half:, lanes]], axis=1)
        decay = jnp.concatenate([whole[:, lanes], whole[:, lanes]], axis=1)
        return wide.astype(bf16), jnp.broadcast_to(decay, (FOLD - half, 2 * HEAD_K)).astype(bf16)

    to_later = folded(forward[count], slice(0, HEAD_K))
    to_earlier = folded(backward[count], slice(HEAD_K, 2 * HEAD_K))
    for peer in range(PEERS):
        later = peer > me
        send_ref[peer, :half] = jnp.where(later, to_later[0], to_earlier[0])
        send_ref[peer, half:] = jnp.where(later, to_later[1], to_earlier[1])


def gate_kernel(pos, got_ref, local_hbm, carry_hbm, gate_hbm, gain_ref, keep_ref, give_ref, both_s, local_ref, carry_ref, gate_ref, sems):
    loads = ((carry_hbm, carry_ref), (local_hbm, local_ref), (gate_hbm, gate_ref))
    loads = [pltpu.make_async_copy(src, dst, sems.at[n]) for n, (src, dst) in enumerate(loads)]
    for load in loads:
        load.start()
    me = pos[0] * 4 + pos[1]
    half = HEAD_V // 2
    fwd = jnp.zeros((half, 2 * HEAD_K), f32)
    bwd = jnp.zeros((half, 2 * HEAD_K), f32)
    for peer in range(PEERS):
        state = got_ref[peer, :half].astype(f32)
        decay = got_ref[peer, half : half + 16].astype(f32)[:1]
        fwd = jnp.where(peer < me, fwd * decay + state, fwd)
    for peer in reversed(range(PEERS)):
        state = got_ref[peer, :half].astype(f32)
        decay = got_ref[peer, half : half + 16].astype(f32)[:1]
        bwd = jnp.where(peer > me, bwd * decay + state, bwd)
    top = jnp.concatenate([fwd[:, :HEAD_K], bwd[:, :HEAD_K]], axis=1)
    low = jnp.concatenate([fwd[:, HEAD_K:], bwd[:, HEAD_K:]], axis=1)
    state = jnp.concatenate([top, low], axis=0).astype(bf16)
    for load in loads:
        load.wait()
    for group in range(8):
        rows = slice(group * ROWS, (group + 1) * ROWS)
        out = local_ref[rows] + dot(carry_ref[rows], state, ((1,), (1,)))
        scale = lax.rsqrt(jnp.mean(out * out, axis=-1, keepdims=True) + norm_eps)
        gate = gate_ref[rows].astype(f32)
        gate = gate / (1.0 + jnp.exp(-gate))
        both_s[lax.bitwise_xor(pos[3], group % 2), group // 2] = (out * scale * gain_ref[...] * gate).astype(bf16)
    keep_ref[...] = both_s[0]
    give_ref[...] = both_s[1]


def mix_kernel(pos, g0, g1, g2, g3, s0, s1, s2, s3, w_hbm, gain_ref, near_ref, far_ref, own_ref, xs, res, w_ref, sems):
    wide = 512
    loads = []
    for n in range(D // wide):
        cols = pl.ds(n * wide, wide)
        loads.append(pltpu.make_async_copy(w_hbm.at[:, cols], w_ref.at[:, cols], sems.at[n]))
    for load in loads:
        load.start()
    first = pos[3] == 0
    for d, g in enumerate((g0, g1, g2, g3)):
        for k in range(4):
            at = lax.rem(pos[2] + (NEAR[k] + 4), 4)
            a, b = g[0, at], g[1, at]
            xs[k * ROWS : (k + 1) * ROWS, d * 256 : d * 256 + 128] = jnp.where(first, a, b)
            xs[k * ROWS : (k + 1) * ROWS, d * 256 + 128 : (d + 1) * 256] = jnp.where(first, b, a)
    squares = jnp.zeros((4 * ROWS, 128), f32)
    for n in range(D // wide):
        cols = slice(n * wide, (n + 1) * wide)
        acc = None
        loads[n].wait()
        for d in range(4):
            at = pl.multiple_of(lax.rem(pos[2] + (NEAR[d] + 4), 4) * 256, 256)
            part = dot(xs[:, d * 256 : (d + 1) * 256], w_ref[pl.ds(at, 256), cols])
            acc = part if acc is None else acc + part
        for k, s in enumerate((s0, s1, s2, s3)):
            rows = slice(k * ROWS, (k + 1) * ROWS)
            res[rows, cols] = (s[:, cols].astype(f32) + acc[rows]).astype(bf16)
        line = res[:, cols].astype(f32)
        line = line * line
        for j in range(wide // 128):
            squares = squares + line[:, j * 128 : (j + 1) * 128]
    scale = lax.rsqrt(jnp.sum(squares, axis=-1, keepdims=True) / D + norm_eps)
    e = 2 * pos[3] - 1
    steps = (0, e, -e, 2)
    for j in range(4):
        for i in range(4):
            sp = lax.rem(pos[0] + steps[j] + 4, 4) * 4 + lax.rem(pos[1] + steps[i] + 4, 4)
            cols = pl.ds(pl.multiple_of(sp * 128, 128), 128)
            line = (res[:, cols].astype(f32) * scale * gain_ref[:, cols]).astype(bf16)
            if j < 3:
                near_ref[:, (4 * j + i) * 128 : (4 * j + i + 1) * 128] = line
            else:
                far_ref[:, i * 128 : (i + 1) * 128] = line
    own_ref[...] = res[:ROWS]


TURNED = (0, 2, 1, 3)


def up_copies(pairs, wu, sems, base):
    copies = []
    for j, pair in enumerate(pairs):
        for half in range(2):
            for i in range(4):
                dst = wu.at[pl.ds((4 * j + i) * 128, 128), pl.ds(half * 1024, 1024)]
                src = pair[half].at[TURNED[i] if half else i]
                copies.append(pltpu.make_async_copy(src, dst, sems.at[base + len(copies)]))
    return copies


def down_copies(pairs, wd, sems, base):
    copies = []
    for j, pair in enumerate(pairs):
        for half in range(2):
            for i in range(4):
                dst = wd.at[pl.ds(half * 1024, 1024), pl.ds(j * 512 + i * 128, 128)]
                src = pair[half].at[TURNED[i] if half else i]
                copies.append(pltpu.make_async_copy(src, dst, sems.at[base + len(copies)]))
    return copies


def up_kernel(x_ref, *refs):
    pairs, (acc_ref, wu, sems) = [refs[2 * j : 2 * j + 2] for j in range(3)], refs[6:]
    copies = up_copies(pairs, wu, sems, 0)
    for copy in copies:
        copy.start()
    for copy in copies:
        copy.wait()
    wide = 512
    for n in range(2048 // wide):
        cols = slice(n * wide, (n + 1) * wide)
        acc_ref[:, cols] = dot(x_ref[...], wu[:, cols])


def turn_kernel(x_ref, acc_ref, u0, u1, d0, d1, hid_ref, o0, o1, o2, o3, wu, wd, sems):
    ups = up_copies([(u0, u1)], wu, sems, 0)
    downs = down_copies([(d0, d1)], wd, sems, 8)
    for copy in ups + downs:
        copy.start()
    for copy in ups:
        copy.wait()
    wide = 512
    for n in range(2048 // wide):
        cols = slice(n * wide, (n + 1) * wide)
        h = jnp.maximum(acc_ref[:, cols] + dot(x_ref[...], wu[:, cols]), 0.0)
        hid_ref[:, cols] = (h * h).astype(bf16)
    for copy in downs:
        copy.wait()
    part = dot(hid_ref[...], wd[...]).astype(bf16)
    for k, o in enumerate((o0, o1, o2, o3)):
        o[...] = part[k * ROWS : (k + 1) * ROWS]


def down_kernel(hid_ref, *refs, count):
    pairs, outs = [refs[2 * j : 2 * j + 2] for j in range(count)], refs[2 * count : 2 * count + 4]
    wd, sems = refs[2 * count + 4 :]
    copies = down_copies(pairs, wd, sems, 0)
    for copy in copies:
        copy.start()
    for j in range(count):
        for copy in copies[8 * j : 8 * j + 8]:
            copy.wait()
        cols = slice(j * 512, (j + 1) * 512)
        part = dot(hid_ref[...], wd[:, cols]).astype(bf16)
        for k, o in enumerate(outs):
            o[:, cols] = part[k * ROWS : (k + 1) * ROWS]


def end_kernel(pos, res_ref, *refs):
    parts, out_ref = [refs[4 * n : 4 * n + 4] for n in range(3)], refs[12]
    e = 2 * pos[3] - 1
    steps = (0, e, -e, 2)
    for j in range(4):
        for i in range(4):
            sp = lax.rem(pos[0] + steps[i] + 4, 4) * 4 + lax.rem(pos[1] + steps[j] + 4, 4)
            at = pl.ds(pl.multiple_of(sp * 128, 128), 128)
            src, off = ((parts[0], 0), (parts[1], 0), (parts[1], 512), (parts[2], 0))[j]
            cols = slice(off + i * 128, off + (i + 1) * 128)
            total = src[0][:, cols].astype(f32) + src[1][:, cols].astype(f32)
            total = total + src[2][:, cols].astype(f32) + src[3][:, cols].astype(f32)
            out_ref[:, at] = (res_ref[:, at].astype(f32) + total).astype(bf16)


def join_kernel(*refs):
    out_ref, sems = refs[4:]
    copies = [pltpu.make_async_copy(refs[i], out_ref.at[i], sems.at[i]) for i in range(4)]
    for copy in copies:
        copy.start()
    for copy in copies:
        copy.wait()


def mark_kernel(pos, out_ref):
    for i in range(4):
        out_ref[i] = pos[i]


def call(kernel, ins, outs, scratch, args, flops, nbytes, limit, spec=VMEM):
    return launched(kernel, ins, outs, scratch, args, flops, nbytes, limit, spec)


def launched(kernel, ins, outs, scratch, args, flops, nbytes, limit, spec):
    return pl.pallas_call(
        kernel,
        in_specs=ins,
        out_specs=[spec] * len(outs),
        out_shape=[jax.ShapeDtypeStruct(s, t) for s, t in outs],
        scratch_shapes=scratch,
        cost_estimate=pl.CostEstimate(flops=flops, bytes_accessed=nbytes, transcendentals=0),
        compiler_params=pltpu.CompilerParams(vmem_limit_bytes=limit * 1024 * 1024),
    )(*args)


def shifted(v, axis, by, n=4):
    return lax.ppermute(v, axis, [(i, (i + by) % n) for i in range(n)])


def swapped(v):
    return lax.ppermute(v, "c", [(0, 1), (1, 0)])


def both_ways(v, axis, sign):
    pairs = [(2 * i + c, 2 * ((i + sign * (1 - 2 * c)) % 4) + c) for i in range(4) for c in range(2)]
    return lax.ppermute(v, (axis, "c"), pairs)


def joined(blocks):
    shape = (4, *blocks[0].shape)
    scratch = [pltpu.SemaphoreType.DMA((4,))]
    return call(join_kernel, [VMEM] * 4, [(shape, bf16)], scratch, blocks, 800_000_000, 2_000_000, 4, HBM)[0]


def local(
    queries,
    keys,
    values,
    out_gate,
    decay_logit,
    head_gain,
    out_weight,
    stream,
    mlp_gain,
    up_weight,
    down_weight,
):
    length = queries.shape[0]
    pos = jnp.stack([lax.axis_index(a) for a in ("z", "y", "x", "c")]).astype(jnp.int32)

    up_a, up_b = both_ways(up_weight, "y", 1), both_ways(up_weight, "y", -1)
    down_a, down_b = both_ways(down_weight, "z", 1), both_ways(down_weight, "z", -1)

    rows_out, carry, sent = call(
        attend_kernel,
        [SMEM] + [VMEM] * 4,
        [((length, HEAD_V), f32), ((length, 2 * HEAD_K), bf16), ((PEERS, FOLD, 128), bf16)],
        [
            pltpu.VMEM((length, 2 * HEAD_K), f32),
            pltpu.VMEM((length // BLOCK, 2 * HEAD_K), f32),
            pltpu.VMEM((length // BLOCK, HEAD_V, 2 * HEAD_K), f32),
        ],
        (pos, queries.T, keys.T, values, decay_logit.transpose(0, 2, 1)),
        2_000_000_000,
        2_000_000,
        60,
    )
    up_2 = both_ways(up_a, "y", 1)
    down_2 = both_ways(down_a, "z", 1)
    streams = [stream] + [shifted(stream, "x", NEAR[k]) for k in (3, 2, 1)]
    streams = [streams[0], streams[2], streams[3], streams[1]]
    got = lax.all_to_all(sent, SP, 0, 0, tiled=True)
    up_line = joined((up_weight, up_a, up_b, up_2))
    down_line = joined((down_weight, down_a, down_b, down_2))
    up_na, up_nb = both_ways(up_line, "z", 1), both_ways(up_line, "z", -1)
    down_na, down_nb = both_ways(down_line, "y", 1), both_ways(down_line, "y", -1)
    up_n2 = both_ways(up_na, "z", 1)
    down_n2 = both_ways(down_na, "y", 1)
    ups = [up_line, up_na, up_nb, up_n2]
    ups_s = [swapped(v) for v in ups]
    downs = [down_line, down_na, down_nb, down_n2]
    downs_s = [swapped(v) for v in downs]
    keep, give = call(
        gate_kernel,
        [SMEM, VMEM, HBM, HBM, HBM, VMEM],
        [((4, ROWS, HEAD_V), bf16)] * 2,
        [
            pltpu.VMEM((2, 4, ROWS, HEAD_V), bf16),
            pltpu.VMEM((length, HEAD_V), f32),
            pltpu.VMEM((length, 2 * HEAD_K), bf16),
            pltpu.VMEM((length, HEAD_V), bf16),
            pltpu.SemaphoreType.DMA((3,)),
        ],
        (pos, got, rows_out, carry, out_gate, head_gain.reshape(1, HEAD_V)),
        1_000_000_000,
        2_000_000,
        8,
    )
    pair = jnp.stack([keep, swapped(give)])
    heads = {k: shifted(pair, "x", NEAR[k]) for k in (1, 2, 3)}
    heads = [pair, heads[2], heads[1], heads[3]]
    pos2 = pl.pallas_call(
        mark_kernel, in_specs=[SMEM], out_specs=SMEM, out_shape=jax.ShapeDtypeStruct((4,), jnp.int32)
    )(pos)
    near, far, residual = call(
        mix_kernel,
        [SMEM] + [VMEM] * 8 + [HBM, VMEM],
        [((4 * ROWS, 1536), bf16), ((4 * ROWS, 512), bf16), ((ROWS, D), bf16)],
        [
            pltpu.VMEM((4 * ROWS, 1024), bf16),
            pltpu.VMEM((4 * ROWS, D), bf16),
            pltpu.VMEM((1024, D), bf16),
            pltpu.SemaphoreType.DMA((4,)),
        ],
        (pos2, *heads, *streams, out_weight, mlp_gain.reshape(1, D)),
        2 * 512 * 1024 * 2048,
        12_000_000,
        24,
    )
    gathered = call(
        up_kernel,
        [VMEM] + [ANY] * 6,
        [((4 * ROWS, 2048), f32)],
        [pltpu.VMEM((1536, 2048), bf16), pltpu.SemaphoreType.DMA((24,))],
        (near, *[w for j in range(3) for w in (ups[j], ups_s[TURNED[j]])]),
        2 * 512 * 1536 * 2048,
        10_000_000,
        20,
    )[0]
    turned = call(
        turn_kernel,
        [VMEM] * 2 + [ANY] * 4,
        [((4 * ROWS, 2048), bf16)] + [((ROWS, 512), bf16)] * 4,
        [pltpu.VMEM((512, 2048), bf16), pltpu.VMEM((2048, 512), bf16), pltpu.SemaphoreType.DMA((16,))],
        (far, gathered, ups[3], ups_s[3], downs[0], downs_s[0]),
        4 * 512 * 512 * 2048,
        8_000_000,
        24,
    )
    hidden, first = turned[0], turned[1:]

    def down(js):
        count = len(js)
        return call(
            functools.partial(down_kernel, count=count),
            [VMEM] + [ANY] * (2 * count),
            [((ROWS, count * 512), bf16)] * 4,
            [pltpu.VMEM((2048, count * 512), bf16), pltpu.SemaphoreType.DMA((8 * count,))],
            (hidden, *[w for j in js for w in (downs[j], downs_s[TURNED[j]])]),
            count * 512 * 2048 * 1024,
            count * 3_000_000,
            20,
        )

    def sent_back(parts):
        return [parts[0]] + [shifted(parts[k], "x", NEAR[k]) for k in (1, 2, 3)]

    first = sent_back(first)
    second = sent_back(down((1, 2)))
    third = sent_back(down((3,)))
    return call(
        end_kernel,
        [SMEM] + [VMEM] * 13,
        [((ROWS, D), bf16)],
        [],
        (pos, residual, *first, *second, *third),
        100_000_000,
        3_000_000,
        8,
    )[0]


def solution(mesh):
    split = Mesh(mesh.devices.reshape(4, 4, 4, 2), ("z", "y", "x", "c"))
    both = SP + TP
    in_specs = (
        P(SP, TP),
        P(SP, TP),
        P(SP, TP),
        P(SP, TP),
        P(None, SP, TP),
        P(TP),
        P(),
        P(both, None),
        P(),
        P(SP, TP),
        P(TP, SP),
    )
    return jax.shard_map(local, mesh=split, in_specs=in_specs, out_specs=P(both, None), check_vma=False)
```

```python
import functools

import jax
import jax.numpy as jnp
from jax import lax
from jax.experimental import pallas as pl
from jax.experimental.pallas import tpu as pltpu
from jax.sharding import Mesh
from jax.sharding import PartitionSpec as P


HEAD_K = 64
HEAD_V = 128
BLOCK = 128
D = 2048
ROWS = 128
SP = ("z", "y")
TP = ("x", "c")
PEERS = 16
FOLD = 80

gate_temper = 16.0
norm_eps = 1e-06
f32 = jnp.float32
bf16 = jnp.bfloat16
NEAR = (0, -1, 1, 2)

VMEM = pl.BlockSpec(memory_space=pltpu.VMEM)
ANY = pl.BlockSpec(memory_space=pl.ANY)
HBM = pl.BlockSpec(memory_space=pltpu.HBM)


def dot(a, b, dims=((1,), (0,)), precision=None):
    return lax.dot_general(a, b, (dims, ((), ())), precision=precision, preferred_element_type=f32)


def position():
    return tuple(lax.axis_index(a) for a in SP + TP)


def attend_kernel(q_ref, k_ref, v_ref, ld_ref, local_ref, carry_ref, send_ref, qd_s, tot_s, inc_s):
    pos = position()
    length = q_ref.shape[1]
    count = length // BLOCK
    me = pos[0] * 4 + pos[1]
    row = lax.broadcasted_iota(jnp.int32, (BLOCK, BLOCK), 0)
    col = lax.broadcasted_iota(jnp.int32, (BLOCK, BLOCK), 1)
    ahead = col < HEAD_K
    lower = jnp.where(row >= col, 1.0, 0.0).astype(bf16)

    for b in range(count):
        rows = slice(b * BLOCK, (b + 1) * BLOCK)
        logit = jnp.concatenate([ld_ref[0, :, rows], ld_ref[1, :, rows]], axis=0).T
        decay = (jnp.minimum(logit, 0.0) - jnp.log1p(jnp.exp(-jnp.abs(logit)))) / gate_temper
        high = decay.astype(bf16)
        low = (decay - high.astype(f32)).astype(bf16)
        run = dot(lower, high) + dot(lower, low)
        total = run[BLOCK - 1 : BLOCK]
        within = jnp.where(ahead, run, total - run + decay)
        grow = jnp.exp(-within)
        q_blk, k_blk = q_ref[:, rows].astype(f32), k_ref[:, rows].astype(f32)
        q2 = jnp.concatenate([q_blk, q_blk], axis=0).T
        k2 = jnp.concatenate([k_blk, k_blk], axis=0).T
        q_dec = q2 * (jnp.exp(within) * HEAD_K ** (-0.5))
        k_inv = k2 * grow
        k_end = (k2 * jnp.exp(total - within)).astype(bf16)
        k_low = k_inv.astype(bf16)
        v_blk = v_ref[rows]
        fwd = dot(jnp.where(ahead, q_dec, 0.0).astype(bf16), k_low, ((1,), (1,)))
        bwd = dot(jnp.where(ahead, 0.0, q_dec).astype(bf16), k_low, ((1,), (1,)))
        scores = jnp.where(row >= col, fwd, 0.0) + jnp.where(row <= col, bwd, 0.0)
        local_ref[rows] = dot(scores.astype(bf16), v_blk)
        inc_s[b] = dot(v_blk, k_end, ((0,), (0,)))
        qd_s[rows] = q_dec
        tot_s[b : b + 1] = total

    totals = [tot_s[b : b + 1] for b in range(count)]
    ends = [jnp.exp(t) for t in totals]
    ahead1 = ahead[:1]
    forward = [jnp.zeros((HEAD_V, 2 * HEAD_K), f32)]
    before = [jnp.zeros_like(totals[0])]
    for b in range(count):
        forward.append(forward[b] * ends[b] + inc_s[b])
        before.append(before[b] + totals[b])
    backward = [jnp.zeros((HEAD_V, 2 * HEAD_K), f32)]
    after = [jnp.zeros_like(totals[0])]
    for b in reversed(range(count)):
        backward.append(backward[-1] * ends[b] + inc_s[b])
        after.append(after[-1] + totals[b])
    for b in range(count):
        rows = slice(b * BLOCK, (b + 1) * BLOCK)
        state = jnp.where(ahead, forward[b], backward[count - 1 - b]).astype(bf16)
        q_dec = qd_s[rows]
        local_ref[rows] = local_ref[rows] + dot(q_dec.astype(bf16), state, ((1,), (1,)))
        reach = jnp.exp(jnp.where(ahead1, before[b], after[count - 1 - b]))
        carry_ref[rows] = (q_dec * reach).astype(bf16)

    whole = jnp.exp(before[count])
    half = HEAD_V // 2

    def folded(state, lanes):
        wide = jnp.concatenate([state[:half, lanes], state[half:, lanes]], axis=1)
        decay = jnp.concatenate([whole[:, lanes], whole[:, lanes]], axis=1)
        return wide.astype(bf16), jnp.broadcast_to(decay, (FOLD - half, 2 * HEAD_K)).astype(bf16)

    to_later = folded(forward[count], slice(0, HEAD_K))
    to_earlier = folded(backward[count], slice(HEAD_K, 2 * HEAD_K))
    for peer in range(PEERS):
        later = peer > me
        send_ref[peer, :half] = jnp.where(later, to_later[0], to_earlier[0])
        send_ref[peer, half:] = jnp.where(later, to_later[1], to_earlier[1])


def gate_kernel(got_ref, local_hbm, carry_hbm, gate_hbm, gain_ref, keep_ref, give_ref, both_s, local_ref, carry_ref, gate_ref, sems):
    pos = position()
    loads = ((carry_hbm, carry_ref), (local_hbm, local_ref), (gate_hbm, gate_ref))
    loads = [pltpu.make_async_copy(src, dst, sems.at[n]) for n, (src, dst) in enumerate(loads)]
    for load in loads:
        load.start()
    me = pos[0] * 4 + pos[1]
    half = HEAD_V // 2
    fwd = jnp.zeros((half, 2 * HEAD_K), f32)
    bwd = jnp.zeros((half, 2 * HEAD_K), f32)
    for peer in range(PEERS):
        state = got_ref[peer, :half].astype(f32)
        decay = got_ref[peer, half : half + 16].astype(f32)[:1]
        fwd = jnp.where(peer < me, fwd * decay + state, fwd)
    for peer in reversed(range(PEERS)):
        state = got_ref[peer, :half].astype(f32)
        decay = got_ref[peer, half : half + 16].astype(f32)[:1]
        bwd = jnp.where(peer > me, bwd * decay + state, bwd)
    top = jnp.concatenate([fwd[:, :HEAD_K], bwd[:, :HEAD_K]], axis=1)
    low = jnp.concatenate([fwd[:, HEAD_K:], bwd[:, HEAD_K:]], axis=1)
    state = jnp.concatenate([top, low], axis=0).astype(bf16)
    for load in loads:
        load.wait()
    for group in range(8):
        rows = slice(group * ROWS, (group + 1) * ROWS)
        out = local_ref[rows] + dot(carry_ref[rows], state, ((1,), (1,)))
        scale = lax.rsqrt(jnp.mean(out * out, axis=-1, keepdims=True) + norm_eps)
        gate = gate_ref[rows].astype(f32)
        gate = gate / (1.0 + jnp.exp(-gate))
        both_s[lax.bitwise_xor(pos[3], group % 2), group // 2] = (out * scale * gain_ref[...] * gate).astype(bf16)
    keep_ref[...] = both_s[0]
    give_ref[...] = both_s[1]


def mix_kernel(g0, g1, g2, g3, s0, s1, s2, s3, w_ref, gain_ref, near_ref, far_ref, own_ref, xs, res):
    pos = position()
    wide = 512
    first = pos[3] == 0
    for d, g in enumerate((g0, g1, g2, g3)):
        for k in range(4):
            at = lax.rem(pos[2] + (NEAR[k] + 4), 4)
            a, b = g[0, at], g[1, at]
            xs[k * ROWS : (k + 1) * ROWS, d * 256 : d * 256 + 128] = jnp.where(first, a, b)
            xs[k * ROWS : (k + 1) * ROWS, d * 256 + 128 : (d + 1) * 256] = jnp.where(first, b, a)
    squares = jnp.zeros((4 * ROWS, 128), f32)
    for n in range(D // wide):
        cols = slice(n * wide, (n + 1) * wide)
        acc = None
        for d in range(4):
            at = pl.multiple_of(lax.rem(pos[2] + (NEAR[d] + 4), 4) * 256, 256)
            part = dot(xs[:, d * 256 : (d + 1) * 256], w_ref[pl.ds(at, 256), cols])
            acc = part if acc is None else acc + part
        for k, s in enumerate((s0, s1, s2, s3)):
            rows = slice(k * ROWS, (k + 1) * ROWS)
            res[rows, cols] = (s[:, cols].astype(f32) + acc[rows]).astype(bf16)
        line = res[:, cols].astype(f32)
        line = line * line
        for j in range(wide // 128):
            squares = squares + line[:, j * 128 : (j + 1) * 128]
    scale = lax.rsqrt(jnp.sum(squares, axis=-1, keepdims=True) / D + norm_eps)
    e = 2 * pos[3] - 1
    steps = (0, e, -e, 2)
    for j in range(4):
        for i in range(4):
            sp = lax.rem(pos[0] + steps[j] + 4, 4) * 4 + lax.rem(pos[1] + steps[i] + 4, 4)
            cols = pl.ds(pl.multiple_of(sp * 128, 128), 128)
            line = (res[:, cols].astype(f32) * scale * gain_ref[:, cols]).astype(bf16)
            if j < 3:
                near_ref[:, (4 * j + i) * 128 : (4 * j + i + 1) * 128] = line
            else:
                far_ref[:, i * 128 : (i + 1) * 128] = line
    own_ref[...] = res[:ROWS]


TURNED = (0, 2, 1, 3)


def up_copies(pairs, wu, sems, base):
    copies = []
    for j, pair in enumerate(pairs):
        for half in range(2):
            for i in range(4):
                dst = wu.at[pl.ds((4 * j + i) * 128, 128), pl.ds(half * 1024, 1024)]
                src = pair[half].at[TURNED[i] if half else i]
                copies.append(pltpu.make_async_copy(src, dst, sems.at[base + len(copies)]))
    return copies


def down_copies(pairs, wd, sems, base):
    copies = []
    for j, pair in enumerate(pairs):
        for half in range(2):
            for i in range(4):
                dst = wd.at[pl.ds(half * 1024, 1024), pl.ds(j * 512 + i * 128, 128)]
                src = pair[half].at[TURNED[i] if half else i]
                copies.append(pltpu.make_async_copy(src, dst, sems.at[base + len(copies)]))
    return copies


def up_kernel(x_ref, *refs):
    pairs, (acc_ref, wu, sems) = [refs[2 * j : 2 * j + 2] for j in range(3)], refs[6:]
    copies = up_copies(pairs, wu, sems, 0)
    for copy in copies:
        copy.start()
    for copy in copies:
        copy.wait()
    wide = 512
    for n in range(2048 // wide):
        cols = slice(n * wide, (n + 1) * wide)
        acc_ref[:, cols] = dot(x_ref[...], wu[:, cols])


def turn_kernel(x_ref, acc_ref, u0, u1, d0, d1, hid_ref, o0, o1, o2, o3, wu, wd, sems):
    ups = up_copies([(u0, u1)], wu, sems, 0)
    downs = down_copies([(d0, d1)], wd, sems, 8)
    for copy in ups + downs:
        copy.start()
    for copy in ups:
        copy.wait()
    wide = 512
    for n in range(2048 // wide):
        cols = slice(n * wide, (n + 1) * wide)
        h = jnp.maximum(acc_ref[:, cols] + dot(x_ref[...], wu[:, cols]), 0.0)
        hid_ref[:, cols] = (h * h).astype(bf16)
    for copy in downs:
        copy.wait()
    part = dot(hid_ref[...], wd[...]).astype(bf16)
    for k, o in enumerate((o0, o1, o2, o3)):
        o[...] = part[k * ROWS : (k + 1) * ROWS]


def down_kernel(hid_ref, *refs, count):
    pairs, outs = [refs[2 * j : 2 * j + 2] for j in range(count)], refs[2 * count : 2 * count + 4]
    wd, sems = refs[2 * count + 4 :]
    copies = down_copies(pairs, wd, sems, 0)
    for copy in copies:
        copy.start()
    for j in range(count):
        for copy in copies[8 * j : 8 * j + 8]:
            copy.wait()
        cols = slice(j * 512, (j + 1) * 512)
        part = dot(hid_ref[...], wd[:, cols]).astype(bf16)
        for k, o in enumerate(outs):
            o[:, cols] = part[k * ROWS : (k + 1) * ROWS]


def end_kernel(res_ref, *refs):
    pos = position()
    parts, out_ref = [refs[4 * n : 4 * n + 4] for n in range(3)], refs[12]
    e = 2 * pos[3] - 1
    steps = (0, e, -e, 2)
    for j in range(4):
        for i in range(4):
            sp = lax.rem(pos[0] + steps[i] + 4, 4) * 4 + lax.rem(pos[1] + steps[j] + 4, 4)
            at = pl.ds(pl.multiple_of(sp * 128, 128), 128)
            src, off = ((parts[0], 0), (parts[1], 0), (parts[1], 512), (parts[2], 0))[j]
            cols = slice(off + i * 128, off + (i + 1) * 128)
            total = src[0][:, cols].astype(f32) + src[1][:, cols].astype(f32)
            total = total + src[2][:, cols].astype(f32) + src[3][:, cols].astype(f32)
            out_ref[:, at] = (res_ref[:, at].astype(f32) + total).astype(bf16)


def relay_kernel(*refs):
    out_ref, held, sems = refs[4:]
    inward = [pltpu.make_async_copy(refs[i], held.at[i], sems.at[i]) for i in range(4)]
    outward = [pltpu.make_async_copy(held.at[i], out_ref.at[i], sems.at[4 + i]) for i in range(4)]
    for copy in inward:
        copy.start()
    for i in range(4):
        inward[i].wait()
        outward[i].start()
    for copy in outward:
        copy.wait()


def join_kernel(*refs):
    out_ref, sems = refs[4:]
    copies = [pltpu.make_async_copy(refs[i], out_ref.at[i], sems.at[i]) for i in range(4)]
    for copy in copies:
        copy.start()
    for copy in copies:
        copy.wait()


def load_kernel(w_ref, out_ref, sem):
    copy = pltpu.make_async_copy(w_ref, out_ref, sem)
    copy.start()
    copy.wait()


def call(kernel, ins, outs, scratch, args, flops, nbytes, limit, spec=VMEM):
    return launched(kernel, ins, outs, scratch, args, flops, nbytes, limit, spec)


def launched(kernel, ins, outs, scratch, args, flops, nbytes, limit, spec):
    return pl.pallas_call(
        kernel,
        in_specs=ins,
        out_specs=[spec] * len(outs),
        out_shape=[jax.ShapeDtypeStruct(s, t) for s, t in outs],
        scratch_shapes=scratch,
        cost_estimate=pl.CostEstimate(flops=flops, bytes_accessed=nbytes, transcendentals=0),
        compiler_params=pltpu.CompilerParams(vmem_limit_bytes=limit * 1024 * 1024),
    )(*args)


def shifted(v, axis, by, n=4):
    return lax.ppermute(v, axis, [(i, (i + by) % n) for i in range(n)])


def swapped(v):
    return lax.ppermute(v, "c", [(0, 1), (1, 0)])


def both_ways(v, axis, sign):
    pairs = [(2 * i + c, 2 * ((i + sign * (1 - 2 * c)) % 4) + c) for i in range(4) for c in range(2)]
    return lax.ppermute(v, (axis, "c"), pairs)


def relayed(blocks):
    shape = (4, *blocks[0].shape)
    scratch = [pltpu.VMEM(shape, bf16), pltpu.SemaphoreType.DMA((8,))]
    return call(relay_kernel, [HBM] * 4, [(shape, bf16)], scratch, blocks, 800_000_000, 2_000_000, 60, HBM)[0]


def joined(blocks):
    shape = (4, *blocks[0].shape)
    scratch = [pltpu.SemaphoreType.DMA((4,))]
    return call(join_kernel, [VMEM] * 4, [(shape, bf16)], scratch, blocks, 800_000_000, 2_000_000, 4, HBM)[0]


def local(
    queries,
    keys,
    values,
    out_gate,
    decay_logit,
    head_gain,
    out_weight,
    stream,
    mlp_gain,
    up_weight,
    down_weight,
):
    length = queries.shape[0]

    up_a, up_b = both_ways(up_weight, "y", 1), both_ways(up_weight, "y", -1)
    down_a, down_b = both_ways(down_weight, "z", 1), both_ways(down_weight, "z", -1)

    rows_out, carry, sent = call(
        attend_kernel,
        [VMEM] * 4,
        [((length, HEAD_V), f32), ((length, 2 * HEAD_K), bf16), ((PEERS, FOLD, 128), bf16)],
        [
            pltpu.VMEM((length, 2 * HEAD_K), f32),
            pltpu.VMEM((length // BLOCK, 2 * HEAD_K), f32),
            pltpu.VMEM((length // BLOCK, HEAD_V, 2 * HEAD_K), f32),
        ],
        (queries.T, keys.T, values, decay_logit.transpose(0, 2, 1)),
        2_000_000_000,
        2_000_000,
        60,
    )
    up_2 = both_ways(up_a, "y", 1)
    down_2 = both_ways(down_a, "z", 1)
    streams = [stream] + [shifted(stream, "x", NEAR[k]) for k in (3, 2, 1)]
    streams = [streams[0], streams[2], streams[3], streams[1]]
    got = lax.all_to_all(sent, SP, 0, 0, tiled=True)
    up_line = joined((up_weight, up_a, up_b, up_2))
    down_line = relayed((down_weight, down_a, down_b, down_2))
    up_na, up_nb = both_ways(up_line, "z", 1), both_ways(up_line, "z", -1)
    down_na, down_nb = both_ways(down_line, "y", 1), both_ways(down_line, "y", -1)
    up_n2 = both_ways(up_na, "z", 1)
    down_n2 = both_ways(down_na, "y", 1)
    ups = [up_line, up_na, up_nb, up_n2]
    ups_s = [swapped(v) for v in ups]
    downs = [down_line, down_na, down_nb, down_n2]
    downs_s = [swapped(v) for v in downs]
    keep, give = call(
        gate_kernel,
        [VMEM, HBM, HBM, HBM, VMEM],
        [((4, ROWS, HEAD_V), bf16)] * 2,
        [
            pltpu.VMEM((2, 4, ROWS, HEAD_V), bf16),
            pltpu.VMEM((length, HEAD_V), f32),
            pltpu.VMEM((length, 2 * HEAD_K), bf16),
            pltpu.VMEM((length, HEAD_V), bf16),
            pltpu.SemaphoreType.DMA((3,)),
        ],
        (got, rows_out, carry, out_gate, head_gain.reshape(1, HEAD_V)),
        1_000_000_000,
        2_000_000,
        60,
    )
    pair = jnp.stack([keep, swapped(give)])
    heads = {k: shifted(pair, "x", NEAR[k]) for k in (1, 2, 3)}
    heads = [pair, heads[2], heads[1], heads[3]]
    mixing = call(
        load_kernel,
        [HBM],
        [(out_weight.shape, bf16)],
        [pltpu.SemaphoreType.DMA],
        (out_weight,),
        1000,
        10000,
        1,
    )[0]
    near, far, residual = call(
        mix_kernel,
        [VMEM] * 10,
        [((4 * ROWS, 1536), bf16), ((4 * ROWS, 512), bf16), ((ROWS, D), bf16)],
        [
            pltpu.VMEM((4 * ROWS, 1024), bf16),
            pltpu.VMEM((4 * ROWS, D), bf16),
        ],
        (*heads, *streams, mixing, mlp_gain.reshape(1, D)),
        2 * 512 * 1024 * 2048,
        12_000_000,
        24,
    )
    gathered = call(
        up_kernel,
        [VMEM] + [ANY] * 6,
        [((4 * ROWS, 2048), f32)],
        [pltpu.VMEM((1536, 2048), bf16), pltpu.SemaphoreType.DMA((24,))],
        (near, *[w for j in range(3) for w in (ups[j], ups_s[TURNED[j]])]),
        2 * 512 * 1536 * 2048,
        10_000_000,
        20,
    )[0]
    turned = call(
        turn_kernel,
        [VMEM] * 2 + [ANY] * 4,
        [((4 * ROWS, 2048), bf16)] + [((ROWS, 512), bf16)] * 4,
        [pltpu.VMEM((512, 2048), bf16), pltpu.VMEM((2048, 512), bf16), pltpu.SemaphoreType.DMA((16,))],
        (far, gathered, ups[3], ups_s[3], downs[0], downs_s[0]),
        4 * 512 * 512 * 2048,
        8_000_000,
        24,
    )
    hidden, first = turned[0], turned[1:]

    def down(js):
        count = len(js)
        return call(
            functools.partial(down_kernel, count=count),
            [VMEM] + [ANY] * (2 * count),
            [((ROWS, count * 512), bf16)] * 4,
            [pltpu.VMEM((2048, count * 512), bf16), pltpu.SemaphoreType.DMA((8 * count,))],
            (hidden, *[w for j in js for w in (downs[j], downs_s[TURNED[j]])]),
            count * 512 * 2048 * 1024,
            count * 3_000_000,
            20,
        )

    def sent_back(parts):
        return [parts[0]] + [shifted(parts[k], "x", NEAR[k]) for k in (1, 2, 3)]

    first = sent_back(first)
    second = sent_back(down((1, 2)))
    third = sent_back(down((3,)))
    return call(
        end_kernel,
        [VMEM] * 13,
        [((ROWS, D), bf16)],
        [],
        (residual, *first, *second, *third),
        100_000_000,
        3_000_000,
        8,
    )[0]


def solution(mesh):
    split = Mesh(mesh.devices.reshape(4, 4, 4, 2), ("z", "y", "x", "c"))
    both = SP + TP
    in_specs = (
        P(SP, TP),
        P(SP, TP),
        P(SP, TP),
        P(SP, TP),
        P(None, SP, TP),
        P(TP),
        P(),
        P(both, None),
        P(),
        P(SP, TP),
        P(TP, SP),
    )
    return jax.shard_map(local, mesh=split, in_specs=in_specs, out_specs=P(both, None), check_vma=False)
```

```python
import functools

import jax
import jax.numpy as jnp
from jax import lax
from jax.experimental import pallas as pl
from jax.experimental.pallas import tpu as pltpu
from jax.sharding import Mesh
from jax.sharding import PartitionSpec as P


HEAD_K = 64
HEAD_V = 128
BLOCK = 128
D = 2048
ROWS = 128
SP = ("z", "y")
TP = ("x", "c")
PEERS = 16
FOLD = 72

gate_temper = 16.0
norm_eps = 1e-06
f32 = jnp.float32
bf16 = jnp.bfloat16
NEAR = (0, -1, 1, 2)

VMEM = pl.BlockSpec(memory_space=pltpu.VMEM)
ANY = pl.BlockSpec(memory_space=pl.ANY)
HBM = pl.BlockSpec(memory_space=pltpu.HBM)


def dot(a, b, dims=((1,), (0,)), precision=None):
    return lax.dot_general(a, b, (dims, ((), ())), precision=precision, preferred_element_type=f32)


def position():
    return tuple(lax.axis_index(a) for a in SP + TP)


def attend_kernel(q_ref, k_ref, v_ref, ld_ref, local_ref, carry_ref, send_ref, qd_s, tot_s, inc_s):
    pos = position()
    length = q_ref.shape[1]
    count = length // BLOCK
    me = pos[0] * 4 + pos[1]
    row = lax.broadcasted_iota(jnp.int32, (BLOCK, BLOCK), 0)
    col = lax.broadcasted_iota(jnp.int32, (BLOCK, BLOCK), 1)
    ahead = col < HEAD_K
    lower = jnp.where(row >= col, 1.0, 0.0).astype(bf16)

    for b in range(count):
        rows = slice(b * BLOCK, (b + 1) * BLOCK)
        logit = jnp.concatenate([ld_ref[0, :, rows], ld_ref[1, :, rows]], axis=0).T
        decay = (jnp.minimum(logit, 0.0) - jnp.log1p(jnp.exp(-jnp.abs(logit)))) / gate_temper
        high = decay.astype(bf16)
        low = (decay - high.astype(f32)).astype(bf16)
        run = dot(lower, high) + dot(lower, low)
        total = run[BLOCK - 1 : BLOCK]
        within = jnp.where(ahead, run, total - run + decay)
        grow = jnp.exp(-within)
        q_blk, k_blk = q_ref[:, rows].astype(f32), k_ref[:, rows].astype(f32)
        q2 = jnp.concatenate([q_blk, q_blk], axis=0).T
        k2 = jnp.concatenate([k_blk, k_blk], axis=0).T
        q_dec = q2 * (jnp.exp(within) * HEAD_K ** (-0.5))
        k_inv = k2 * grow
        k_end = (k2 * jnp.exp(total - within)).astype(bf16)
        k_low = k_inv.astype(bf16)
        v_blk = v_ref[rows]
        fwd = dot(jnp.where(ahead, q_dec, 0.0).astype(bf16), k_low, ((1,), (1,)))
        bwd = dot(jnp.where(ahead, 0.0, q_dec).astype(bf16), k_low, ((1,), (1,)))
        scores = jnp.where(row >= col, fwd, 0.0) + jnp.where(row <= col, bwd, 0.0)
        local_ref[rows] = dot(scores.astype(bf16), v_blk)
        inc_s[b] = dot(v_blk, k_end, ((0,), (0,)))
        qd_s[rows] = q_dec
        tot_s[b : b + 1] = total

    totals = [tot_s[b : b + 1] for b in range(count)]
    ends = [jnp.exp(t) for t in totals]
    ahead1 = ahead[:1]
    forward = [jnp.zeros((HEAD_V, 2 * HEAD_K), f32)]
    before = [jnp.zeros_like(totals[0])]
    for b in range(count):
        forward.append(forward[b] * ends[b] + inc_s[b])
        before.append(before[b] + totals[b])
    backward = [jnp.zeros((HEAD_V, 2 * HEAD_K), f32)]
    after = [jnp.zeros_like(totals[0])]
    for b in reversed(range(count)):
        backward.append(backward[-1] * ends[b] + inc_s[b])
        after.append(after[-1] + totals[b])
    for b in range(count):
        rows = slice(b * BLOCK, (b + 1) * BLOCK)
        state = jnp.where(ahead, forward[b], backward[count - 1 - b]).astype(bf16)
        q_dec = qd_s[rows]
        local_ref[rows] = local_ref[rows] + dot(q_dec.astype(bf16), state, ((1,), (1,)))
        reach = jnp.exp(jnp.where(ahead1, before[b], after[count - 1 - b]))
        carry_ref[rows] = (q_dec * reach).astype(bf16)

    whole = jnp.exp(before[count])
    half = HEAD_V // 2

    def folded(state, lanes):
        wide = jnp.concatenate([state[:half, lanes], state[half:, lanes]], axis=1)
        decay = jnp.concatenate([whole[:, lanes], whole[:, lanes]], axis=1)
        return wide.astype(bf16), jnp.broadcast_to(decay, (FOLD - half, 2 * HEAD_K)).astype(bf16)

    to_later = folded(forward[count], slice(0, HEAD_K))
    to_earlier = folded(backward[count], slice(HEAD_K, 2 * HEAD_K))
    for peer in range(PEERS):
        later = peer > me
        send_ref[peer, :half] = jnp.where(later, to_later[0], to_earlier[0])
        send_ref[peer, half:] = jnp.where(later, to_later[1], to_earlier[1])


def gate_kernel(got_ref, local_hbm, carry_hbm, gate_hbm, gain_ref, keep_ref, give_ref, both_s, local_ref, carry_ref, gate_ref, sems):
    pos = position()
    loads = ((carry_hbm, carry_ref), (local_hbm, local_ref), (gate_hbm, gate_ref))
    loads = [pltpu.make_async_copy(src, dst, sems.at[n]) for n, (src, dst) in enumerate(loads)]
    for load in loads:
        load.start()
    me = pos[0] * 4 + pos[1]
    half = HEAD_V // 2
    fwd = jnp.zeros((half, 2 * HEAD_K), f32)
    bwd = jnp.zeros((half, 2 * HEAD_K), f32)
    for peer in range(PEERS):
        state = got_ref[peer, :half].astype(f32)
        decay = got_ref[peer, half : half + 8].astype(f32)[:1]
        fwd = jnp.where(peer < me, fwd * decay + state, fwd)
    for peer in reversed(range(PEERS)):
        state = got_ref[peer, :half].astype(f32)
        decay = got_ref[peer, half : half + 8].astype(f32)[:1]
        bwd = jnp.where(peer > me, bwd * decay + state, bwd)
    top = jnp.concatenate([fwd[:, :HEAD_K], bwd[:, :HEAD_K]], axis=1)
    low = jnp.concatenate([fwd[:, HEAD_K:], bwd[:, HEAD_K:]], axis=1)
    state = jnp.concatenate([top, low], axis=0).astype(bf16)
    for load in loads:
        load.wait()
    for group in range(8):
        rows = slice(group * ROWS, (group + 1) * ROWS)
        out = local_ref[rows] + dot(carry_ref[rows], state, ((1,), (1,)))
        scale = lax.rsqrt(jnp.mean(out * out, axis=-1, keepdims=True) + norm_eps)
        gate = gate_ref[rows].astype(f32)
        gate = gate / (1.0 + jnp.exp(-gate))
        both_s[lax.bitwise_xor(pos[3], group % 2), group // 2] = (out * scale * gain_ref[...] * gate).astype(bf16)
    keep_ref[...] = both_s[0]
    give_ref[...] = both_s[1]


def mix_kernel(g0, g1, g2, g3, s0, s1, s2, s3, w_ref, gain_ref, near_ref, far_ref, own_ref, xs, res):
    pos = position()
    wide = 512
    first = pos[3] == 0
    for d, g in enumerate((g0, g1, g2, g3)):
        for k in range(4):
            at = lax.rem(pos[2] + (NEAR[k] + 4), 4)
            a, b = g[0, at], g[1, at]
            xs[k * ROWS : (k + 1) * ROWS, d * 256 : d * 256 + 128] = jnp.where(first, a, b)
            xs[k * ROWS : (k + 1) * ROWS, d * 256 + 128 : (d + 1) * 256] = jnp.where(first, b, a)
    squares = jnp.zeros((4 * ROWS, 128), f32)
    for n in range(D // wide):
        cols = slice(n * wide, (n + 1) * wide)
        acc = None
        for d in range(4):
            at = pl.multiple_of(lax.rem(pos[2] + (NEAR[d] + 4), 4) * 256, 256)
            part = dot(xs[:, d * 256 : (d + 1) * 256], w_ref[pl.ds(at, 256), cols])
            acc = part if acc is None else acc + part
        for k, s in enumerate((s0, s1, s2, s3)):
            rows = slice(k * ROWS, (k + 1) * ROWS)
            res[rows, cols] = (s[:, cols].astype(f32) + acc[rows]).astype(bf16)
        line = res[:, cols].astype(f32)
        line = line * line
        for j in range(wide // 128):
            squares = squares + line[:, j * 128 : (j + 1) * 128]
    scale = lax.rsqrt(jnp.sum(squares, axis=-1, keepdims=True) / D + norm_eps)
    e = 2 * pos[3] - 1
    steps = (0, e, -e, 2)
    for j in range(4):
        for i in range(4):
            sp = lax.rem(pos[0] + steps[j] + 4, 4) * 4 + lax.rem(pos[1] + steps[i] + 4, 4)
            cols = pl.ds(pl.multiple_of(sp * 128, 128), 128)
            line = (res[:, cols].astype(f32) * scale * gain_ref[:, cols]).astype(bf16)
            if j < 3:
                near_ref[:, (4 * j + i) * 128 : (4 * j + i + 1) * 128] = line
            else:
                far_ref[:, i * 128 : (i + 1) * 128] = line
    own_ref[...] = res[:ROWS]


TURNED = (0, 2, 1, 3)


def up_copies(pairs, wu, sems, base):
    copies = []
    for j, pair in enumerate(pairs):
        for half in range(2):
            for i in range(4):
                dst = wu.at[pl.ds((4 * j + i) * 128, 128), pl.ds(half * 1024, 1024)]
                src = pair[half].at[TURNED[i] if half else i]
                copies.append(pltpu.make_async_copy(src, dst, sems.at[base + len(copies)]))
    return copies


def down_copies(pairs, wd, sems, base):
    copies = []
    for j, pair in enumerate(pairs):
        for half in range(2):
            for i in range(4):
                dst = wd.at[pl.ds(half * 1024, 1024), pl.ds(j * 512 + i * 128, 128)]
                src = pair[half].at[TURNED[i] if half else i]
                copies.append(pltpu.make_async_copy(src, dst, sems.at[base + len(copies)]))
    return copies


def up_kernel(x_ref, *refs):
    pairs, (acc_ref, wu, sems) = [refs[2 * j : 2 * j + 2] for j in range(3)], refs[6:]
    copies = up_copies(pairs, wu, sems, 0)
    for copy in copies:
        copy.start()
    for copy in copies:
        copy.wait()
    wide = 512
    for n in range(2048 // wide):
        cols = slice(n * wide, (n + 1) * wide)
        acc_ref[:, cols] = dot(x_ref[...], wu[:, cols])


def turn_kernel(x_ref, acc_ref, u0, u1, d0, d1, hid_ref, o0, o1, o2, o3, wu, wd, sems):
    ups = up_copies([(u0, u1)], wu, sems, 0)
    downs = down_copies([(d0, d1)], wd, sems, 8)
    for copy in ups + downs:
        copy.start()
    for copy in ups:
        copy.wait()
    wide = 512
    for n in range(2048 // wide):
        cols = slice(n * wide, (n + 1) * wide)
        h = jnp.maximum(acc_ref[:, cols] + dot(x_ref[...], wu[:, cols]), 0.0)
        hid_ref[:, cols] = (h * h).astype(bf16)
    for copy in downs:
        copy.wait()
    part = dot(hid_ref[...], wd[...]).astype(bf16)
    for k, o in enumerate((o0, o1, o2, o3)):
        o[...] = part[k * ROWS : (k + 1) * ROWS]


def down_kernel(hid_ref, *refs, count):
    pairs, outs = [refs[2 * j : 2 * j + 2] for j in range(count)], refs[2 * count : 2 * count + 4]
    wd, sems = refs[2 * count + 4 :]
    copies = down_copies(pairs, wd, sems, 0)
    for copy in copies:
        copy.start()
    for j in range(count):
        for copy in copies[8 * j : 8 * j + 8]:
            copy.wait()
        cols = slice(j * 512, (j + 1) * 512)
        part = dot(hid_ref[...], wd[:, cols]).astype(bf16)
        for k, o in enumerate(outs):
            o[:, cols] = part[k * ROWS : (k + 1) * ROWS]


def end_kernel(res_ref, *refs):
    pos = position()
    parts, out_ref = [refs[4 * n : 4 * n + 4] for n in range(3)], refs[12]
    e = 2 * pos[3] - 1
    steps = (0, e, -e, 2)
    for j in range(4):
        for i in range(4):
            sp = lax.rem(pos[0] + steps[i] + 4, 4) * 4 + lax.rem(pos[1] + steps[j] + 4, 4)
            at = pl.ds(pl.multiple_of(sp * 128, 128), 128)
            src, off = ((parts[0], 0), (parts[1], 0), (parts[1], 512), (parts[2], 0))[j]
            cols = slice(off + i * 128, off + (i + 1) * 128)
            total = src[0][:, cols].astype(f32) + src[1][:, cols].astype(f32)
            total = total + src[2][:, cols].astype(f32) + src[3][:, cols].astype(f32)
            out_ref[:, at] = (res_ref[:, at].astype(f32) + total).astype(bf16)


def relay_kernel(*refs):
    out_ref, held, sems = refs[4:]
    inward = [pltpu.make_async_copy(refs[i], held.at[i], sems.at[i]) for i in range(4)]
    outward = [pltpu.make_async_copy(held.at[i], out_ref.at[i], sems.at[4 + i]) for i in range(4)]
    for copy in inward:
        copy.start()
    for i in range(4):
        inward[i].wait()
        outward[i].start()
    for copy in outward:
        copy.wait()


def join_kernel(*refs):
    out_ref, sems = refs[4:]
    copies = [pltpu.make_async_copy(refs[i], out_ref.at[i], sems.at[i]) for i in range(4)]
    for copy in copies:
        copy.start()
    for copy in copies:
        copy.wait()


def load_kernel(w_ref, out_ref, sem):
    copy = pltpu.make_async_copy(w_ref, out_ref, sem)
    copy.start()
    copy.wait()


def call(kernel, ins, outs, scratch, args, flops, nbytes, limit, spec=VMEM):
    return launched(kernel, ins, outs, scratch, args, flops, nbytes, limit, spec)


def launched(kernel, ins, outs, scratch, args, flops, nbytes, limit, spec):
    return pl.pallas_call(
        kernel,
        in_specs=ins,
        out_specs=[spec] * len(outs),
        out_shape=[jax.ShapeDtypeStruct(s, t) for s, t in outs],
        scratch_shapes=scratch,
        cost_estimate=pl.CostEstimate(flops=flops, bytes_accessed=nbytes, transcendentals=0),
        compiler_params=pltpu.CompilerParams(vmem_limit_bytes=limit * 1024 * 1024),
    )(*args)


def shifted(v, axis, by, n=4):
    return lax.ppermute(v, axis, [(i, (i + by) % n) for i in range(n)])


def swapped(v):
    return lax.ppermute(v, "c", [(0, 1), (1, 0)])


def both_ways(v, axis, sign):
    pairs = [(2 * i + c, 2 * ((i + sign * (1 - 2 * c)) % 4) + c) for i in range(4) for c in range(2)]
    return lax.ppermute(v, (axis, "c"), pairs)


def relayed(blocks):
    shape = (4, *blocks[0].shape)
    scratch = [pltpu.VMEM(shape, bf16), pltpu.SemaphoreType.DMA((8,))]
    return call(relay_kernel, [HBM] * 4, [(shape, bf16)], scratch, blocks, 800_000_000, 2_000_000, 60, HBM)[0]


def joined(blocks):
    shape = (4, *blocks[0].shape)
    scratch = [pltpu.SemaphoreType.DMA((4,))]
    return call(join_kernel, [VMEM] * 4, [(shape, bf16)], scratch, blocks, 800_000_000, 2_000_000, 4, HBM)[0]


def local(
    queries,
    keys,
    values,
    out_gate,
    decay_logit,
    head_gain,
    out_weight,
    stream,
    mlp_gain,
    up_weight,
    down_weight,
):
    length = queries.shape[0]

    up_a, up_b = both_ways(up_weight, "y", 1), both_ways(up_weight, "y", -1)
    down_a, down_b = both_ways(down_weight, "z", 1), both_ways(down_weight, "z", -1)

    rows_out, carry, sent = call(
        attend_kernel,
        [VMEM] * 4,
        [((length, HEAD_V), f32), ((length, 2 * HEAD_K), bf16), ((PEERS, FOLD, 128), bf16)],
        [
            pltpu.VMEM((length, 2 * HEAD_K), f32),
            pltpu.VMEM((length // BLOCK, 2 * HEAD_K), f32),
            pltpu.VMEM((length // BLOCK, HEAD_V, 2 * HEAD_K), f32),
        ],
        (queries.T, keys.T, values, decay_logit.transpose(0, 2, 1)),
        2_000_000_000,
        2_000_000,
        60,
    )
    up_2 = both_ways(up_a, "y", 1)
    down_2 = both_ways(down_a, "z", 1)
    streams = [stream] + [shifted(stream, "x", NEAR[k]) for k in (3, 2, 1)]
    streams = [streams[0], streams[2], streams[3], streams[1]]
    got = lax.all_to_all(sent, SP, 0, 0, tiled=True)
    up_line = joined((up_weight, up_a, up_b, up_2))
    down_line = relayed((down_weight, down_a, down_b, down_2))
    up_na, up_nb = both_ways(up_line, "z", 1), both_ways(up_line, "z", -1)
    down_na, down_nb = both_ways(down_line, "y", 1), both_ways(down_line, "y", -1)
    up_n2 = both_ways(up_na, "z", 1)
    down_n2 = both_ways(down_na, "y", 1)
    ups = [up_line, up_na, up_nb, up_n2]
    ups_s = [swapped(v) for v in ups]
    downs = [down_line, down_na, down_nb, down_n2]
    downs_s = [swapped(v) for v in downs]
    keep, give = call(
        gate_kernel,
        [VMEM, HBM, HBM, HBM, VMEM],
        [((4, ROWS, HEAD_V), bf16)] * 2,
        [
            pltpu.VMEM((2, 4, ROWS, HEAD_V), bf16),
            pltpu.VMEM((length, HEAD_V), f32),
            pltpu.VMEM((length, 2 * HEAD_K), bf16),
            pltpu.VMEM((length, HEAD_V), bf16),
            pltpu.SemaphoreType.DMA((3,)),
        ],
        (got, rows_out, carry, out_gate, head_gain.reshape(1, HEAD_V)),
        1_000_000_000,
        2_000_000,
        60,
    )
    pair = jnp.stack([keep, swapped(give)])
    heads = {k: shifted(pair, "x", NEAR[k]) for k in (1, 2, 3)}
    heads = [pair, heads[2], heads[1], heads[3]]
    mixing = call(
        load_kernel,
        [HBM],
        [(out_weight.shape, bf16)],
        [pltpu.SemaphoreType.DMA],
        (out_weight,),
        1000,
        10000,
        1,
    )[0]
    near, far, residual = call(
        mix_kernel,
        [VMEM] * 10,
        [((4 * ROWS, 1536), bf16), ((4 * ROWS, 512), bf16), ((ROWS, D), bf16)],
        [
            pltpu.VMEM((4 * ROWS, 1024), bf16),
            pltpu.VMEM((4 * ROWS, D), bf16),
        ],
        (*heads, *streams, mixing, mlp_gain.reshape(1, D)),
        2 * 512 * 1024 * 2048,
        12_000_000,
        24,
    )
    gathered = call(
        up_kernel,
        [VMEM] + [ANY] * 6,
        [((4 * ROWS, 2048), f32)],
        [pltpu.VMEM((1536, 2048), bf16), pltpu.SemaphoreType.DMA((24,))],
        (near, *[w for j in range(3) for w in (ups[j], ups_s[TURNED[j]])]),
        2 * 512 * 1536 * 2048,
        10_000_000,
        20,
    )[0]
    turned = call(
        turn_kernel,
        [VMEM] * 2 + [ANY] * 4,
        [((4 * ROWS, 2048), bf16)] + [((ROWS, 512), bf16)] * 4,
        [pltpu.VMEM((512, 2048), bf16), pltpu.VMEM((2048, 512), bf16), pltpu.SemaphoreType.DMA((16,))],
        (far, gathered, ups[3], ups_s[3], downs[0], downs_s[0]),
        4 * 512 * 512 * 2048,
        8_000_000,
        24,
    )
    hidden, first = turned[0], turned[1:]

    def down(js):
        count = len(js)
        return call(
            functools.partial(down_kernel, count=count),
            [VMEM] + [ANY] * (2 * count),
            [((ROWS, count * 512), bf16)] * 4,
            [pltpu.VMEM((2048, count * 512), bf16), pltpu.SemaphoreType.DMA((8 * count,))],
            (hidden, *[w for j in js for w in (downs[j], downs_s[TURNED[j]])]),
            count * 512 * 2048 * 1024,
            count * 3_000_000,
            20,
        )

    def sent_back(parts):
        return [parts[0]] + [shifted(parts[k], "x", NEAR[k]) for k in (1, 2, 3)]

    first = sent_back(first)
    second = sent_back(down((1, 2)))
    third = sent_back(down((3,)))
    return call(
        end_kernel,
        [VMEM] * 13,
        [((ROWS, D), bf16)],
        [],
        (residual, *first, *second, *third),
        100_000_000,
        3_000_000,
        8,
    )[0]


def solution(mesh):
    split = Mesh(mesh.devices.reshape(4, 4, 4, 2), ("z", "y", "x", "c"))
    both = SP + TP
    in_specs = (
        P(SP, TP),
        P(SP, TP),
        P(SP, TP),
        P(SP, TP),
        P(None, SP, TP),
        P(TP),
        P(),
        P(both, None),
        P(),
        P(SP, TP),
        P(TP, SP),
    )
    return jax.shard_map(local, mesh=split, in_specs=in_specs, out_specs=P(both, None), check_vma=False)
```

```python
import functools

import jax
import jax.numpy as jnp
from jax import lax
from jax.experimental import pallas as pl
from jax.experimental.pallas import tpu as pltpu
from jax.sharding import Mesh
from jax.sharding import PartitionSpec as P


HEAD_K = 64
HEAD_V = 128
BLOCK = 128
D = 2048
ROWS = 128
SP = ("z", "y")
TP = ("x", "c")
PEERS = 16
FOLD = 72

gate_temper = 16.0
norm_eps = 1e-06
f32 = jnp.float32
bf16 = jnp.bfloat16
NEAR = (0, -1, 1, 2)

VMEM = pl.BlockSpec(memory_space=pltpu.VMEM)
ANY = pl.BlockSpec(memory_space=pl.ANY)
HBM = pl.BlockSpec(memory_space=pltpu.HBM)


def dot(a, b, dims=((1,), (0,)), precision=None):
    return lax.dot_general(a, b, (dims, ((), ())), precision=precision, preferred_element_type=f32)


def position():
    return tuple(lax.axis_index(a) for a in SP + TP)


def attend_kernel(q_ref, k_ref, v_ref, ld_ref, local_ref, carry_ref, send_ref, qd_s, tot_s, inc_s):
    pos = position()
    length = q_ref.shape[1]
    count = length // BLOCK
    me = pos[0] * 4 + pos[1]
    row = lax.broadcasted_iota(jnp.int32, (BLOCK, BLOCK), 0)
    col = lax.broadcasted_iota(jnp.int32, (BLOCK, BLOCK), 1)
    ahead = col < HEAD_K
    lower = jnp.where(row >= col, 1.0, 0.0).astype(bf16)

    for b in range(count):
        rows = slice(b * BLOCK, (b + 1) * BLOCK)
        logit = jnp.concatenate([ld_ref[0, :, rows], ld_ref[1, :, rows]], axis=0).T
        decay = (jnp.minimum(logit, 0.0) - jnp.log1p(jnp.exp(-jnp.abs(logit)))) / gate_temper
        high = decay.astype(bf16)
        low = (decay - high.astype(f32)).astype(bf16)
        run = dot(lower, high) + dot(lower, low)
        total = run[BLOCK - 1 : BLOCK]
        within = jnp.where(ahead, run, total - run + decay)
        grow = jnp.exp(-within)
        q_blk, k_blk = q_ref[:, rows].astype(f32), k_ref[:, rows].astype(f32)
        q2 = jnp.concatenate([q_blk, q_blk], axis=0).T
        k2 = jnp.concatenate([k_blk, k_blk], axis=0).T
        q_dec = q2 * (jnp.exp(within) * HEAD_K ** (-0.5))
        k_inv = k2 * grow
        k_end = (k2 * jnp.exp(total - within)).astype(bf16)
        k_low = k_inv.astype(bf16)
        v_blk = v_ref[rows]
        fwd = dot(jnp.where(ahead, q_dec, 0.0).astype(bf16), k_low, ((1,), (1,)))
        bwd = dot(jnp.where(ahead, 0.0, q_dec).astype(bf16), k_low, ((1,), (1,)))
        scores = jnp.where(row >= col, fwd, 0.0) + jnp.where(row <= col, bwd, 0.0)
        local_ref[rows] = dot(scores.astype(bf16), v_blk)
        inc_s[b] = dot(v_blk, k_end, ((0,), (0,)))
        qd_s[rows] = q_dec
        tot_s[b : b + 1] = total

    totals = [tot_s[b : b + 1] for b in range(count)]
    ends = [jnp.exp(t) for t in totals]
    ahead1 = ahead[:1]
    forward = [jnp.zeros((HEAD_V, 2 * HEAD_K), f32)]
    before = [jnp.zeros_like(totals[0])]
    for b in range(count):
        forward.append(forward[b] * ends[b] + inc_s[b])
        before.append(before[b] + totals[b])
    backward = [jnp.zeros((HEAD_V, 2 * HEAD_K), f32)]
    after = [jnp.zeros_like(totals[0])]
    for b in reversed(range(count)):
        backward.append(backward[-1] * ends[b] + inc_s[b])
        after.append(after[-1] + totals[b])
    for b in range(count):
        rows = slice(b * BLOCK, (b + 1) * BLOCK)
        state = jnp.where(ahead, forward[b], backward[count - 1 - b]).astype(bf16)
        q_dec = qd_s[rows]
        local_ref[rows] = local_ref[rows] + dot(q_dec.astype(bf16), state, ((1,), (1,)))
        reach = jnp.exp(jnp.where(ahead1, before[b], after[count - 1 - b]))
        carry_ref[rows] = (q_dec * reach).astype(bf16)

    whole = jnp.exp(before[count])
    half = HEAD_V // 2

    def folded(state, lanes):
        wide = jnp.concatenate([state[:half, lanes], state[half:, lanes]], axis=1)
        decay = jnp.concatenate([whole[:, lanes], whole[:, lanes]], axis=1)
        return wide.astype(bf16), jnp.broadcast_to(decay, (FOLD - half, 2 * HEAD_K)).astype(bf16)

    to_later = folded(forward[count], slice(0, HEAD_K))
    to_earlier = folded(backward[count], slice(HEAD_K, 2 * HEAD_K))
    for peer in range(PEERS):
        later = peer > me
        send_ref[peer, :half] = jnp.where(later, to_later[0], to_earlier[0])
        send_ref[peer, half:] = jnp.where(later, to_later[1], to_earlier[1])


def gate_kernel(got_ref, local_hbm, carry_hbm, gate_hbm, gain_ref, keep_ref, give_ref, both_s, local_ref, carry_ref, gate_ref, sems):
    pos = position()
    loads = ((carry_hbm, carry_ref), (local_hbm, local_ref), (gate_hbm, gate_ref))
    loads = [pltpu.make_async_copy(src, dst, sems.at[n]) for n, (src, dst) in enumerate(loads)]
    for load in loads:
        load.start()
    me = pos[0] * 4 + pos[1]
    half = HEAD_V // 2
    fwd = jnp.zeros((half, 2 * HEAD_K), f32)
    bwd = jnp.zeros((half, 2 * HEAD_K), f32)
    for peer in range(PEERS):
        state = got_ref[peer, :half].astype(f32)
        decay = got_ref[peer, half : half + 8].astype(f32)[:1]
        fwd = jnp.where(peer < me, fwd * decay + state, fwd)
    for peer in reversed(range(PEERS)):
        state = got_ref[peer, :half].astype(f32)
        decay = got_ref[peer, half : half + 8].astype(f32)[:1]
        bwd = jnp.where(peer > me, bwd * decay + state, bwd)
    top = jnp.concatenate([fwd[:, :HEAD_K], bwd[:, :HEAD_K]], axis=1)
    low = jnp.concatenate([fwd[:, HEAD_K:], bwd[:, HEAD_K:]], axis=1)
    state = jnp.concatenate([top, low], axis=0).astype(bf16)
    for load in loads:
        load.wait()
    for group in range(8):
        rows = slice(group * ROWS, (group + 1) * ROWS)
        out = local_ref[rows] + dot(carry_ref[rows], state, ((1,), (1,)))
        scale = lax.rsqrt(jnp.mean(out * out, axis=-1, keepdims=True) + norm_eps)
        gate = gate_ref[rows].astype(f32)
        gate = gate / (1.0 + jnp.exp(-gate))
        both_s[lax.bitwise_xor(pos[3], group % 2), group // 2] = (out * scale * gain_ref[...] * gate).astype(bf16)
    keep_ref[...] = both_s[0]
    give_ref[...] = both_s[1]


def mix_kernel(g0, g1, g2, g3, s0, s1, s2, s3, w_ref, gain_ref, near_ref, far_ref, own_ref, xs, res):
    pos = position()
    wide = 512
    first = pos[3] == 0
    for d, g in enumerate((g0, g1, g2, g3)):
        for k in range(4):
            at = lax.rem(pos[2] + (NEAR[k] + 4), 4)
            a, b = g[0, at], g[1, at]
            xs[k * ROWS : (k + 1) * ROWS, d * 256 : d * 256 + 128] = jnp.where(first, a, b)
            xs[k * ROWS : (k + 1) * ROWS, d * 256 + 128 : (d + 1) * 256] = jnp.where(first, b, a)
    squares = jnp.zeros((4 * ROWS, 128), f32)
    for n in range(D // wide):
        cols = slice(n * wide, (n + 1) * wide)
        acc = None
        for d in range(4):
            at = pl.multiple_of(lax.rem(pos[2] + (NEAR[d] + 4), 4) * 256, 256)
            part = dot(xs[:, d * 256 : (d + 1) * 256], w_ref[pl.ds(at, 256), cols])
            acc = part if acc is None else acc + part
        for k, s in enumerate((s0, s1, s2, s3)):
            rows = slice(k * ROWS, (k + 1) * ROWS)
            res[rows, cols] = (s[:, cols].astype(f32) + acc[rows]).astype(bf16)
        line = res[:, cols].astype(f32)
        line = line * line
        for j in range(wide // 128):
            squares = squares + line[:, j * 128 : (j + 1) * 128]
    scale = lax.rsqrt(jnp.sum(squares, axis=-1, keepdims=True) / D + norm_eps)
    e = 2 * pos[3] - 1
    steps = (0, e, -e, 2)
    for j in range(4):
        for i in range(4):
            sp = lax.rem(pos[0] + steps[j] + 4, 4) * 4 + lax.rem(pos[1] + steps[i] + 4, 4)
            cols = pl.ds(pl.multiple_of(sp * 128, 128), 128)
            line = (res[:, cols].astype(f32) * scale * gain_ref[:, cols]).astype(bf16)
            if j < 3:
                near_ref[:, (4 * j + i) * 128 : (4 * j + i + 1) * 128] = line
            else:
                far_ref[:, i * 128 : (i + 1) * 128] = line
    own_ref[...] = res[:ROWS]


TURNED = (0, 2, 1, 3)


def up_copies(pairs, wu, sems, base):
    copies = []
    for j, pair in enumerate(pairs):
        for half in range(2):
            for i in range(4):
                dst = wu.at[pl.ds((4 * j + i) * 128, 128), pl.ds(half * 1024, 1024)]
                src = pair[half].at[TURNED[i] if half else i]
                copies.append(pltpu.make_async_copy(src, dst, sems.at[base + len(copies)]))
    return copies


def down_copies(pairs, wd, sems, base):
    copies = []
    for j, pair in enumerate(pairs):
        for half in range(2):
            for i in range(4):
                dst = wd.at[pl.ds(half * 1024, 1024), pl.ds(j * 512 + i * 128, 128)]
                src = pair[half].at[TURNED[i] if half else i]
                copies.append(pltpu.make_async_copy(src, dst, sems.at[base + len(copies)]))
    return copies


def up_kernel(x_ref, *refs):
    pairs, (acc_ref, wu, sems) = [refs[2 * j : 2 * j + 2] for j in range(3)], refs[6:]
    copies = up_copies(pairs, wu, sems, 0)
    for copy in copies:
        copy.start()
    for copy in copies:
        copy.wait()
    wide = 512
    for n in range(2048 // wide):
        cols = slice(n * wide, (n + 1) * wide)
        acc_ref[:, cols] = dot(x_ref[...], wu[:, cols])


def turn_kernel(x_ref, acc_ref, u0, u1, d0, d1, hid_ref, o0, o1, o2, o3, wu, wd, sems):
    ups = up_copies([(u0, u1)], wu, sems, 0)
    downs = down_copies([(d0, d1)], wd, sems, 8)
    for copy in ups + downs:
        copy.start()
    for copy in ups:
        copy.wait()
    wide = 512
    for n in range(2048 // wide):
        cols = slice(n * wide, (n + 1) * wide)
        h = jnp.maximum(acc_ref[:, cols] + dot(x_ref[...], wu[:, cols]), 0.0)
        hid_ref[:, cols] = (h * h).astype(bf16)
    for copy in downs:
        copy.wait()
    part = dot(hid_ref[...], wd[...]).astype(bf16)
    for k, o in enumerate((o0, o1, o2, o3)):
        o[...] = part[k * ROWS : (k + 1) * ROWS]


def down_kernel(hid_ref, *refs, count):
    pairs, outs = [refs[2 * j : 2 * j + 2] for j in range(count)], refs[2 * count : 2 * count + 4]
    wd, sems = refs[2 * count + 4 :]
    copies = down_copies(pairs, wd, sems, 0)
    for copy in copies:
        copy.start()
    for j in range(count):
        for copy in copies[8 * j : 8 * j + 8]:
            copy.wait()
        cols = slice(j * 512, (j + 1) * 512)
        part = dot(hid_ref[...], wd[:, cols]).astype(bf16)
        for k, o in enumerate(outs):
            o[:, cols] = part[k * ROWS : (k + 1) * ROWS]


def end_kernel(res_ref, *refs):
    pos = position()
    parts, out_ref = [refs[4 * n : 4 * n + 4] for n in range(3)], refs[12]
    e = 2 * pos[3] - 1
    steps = (0, e, -e, 2)
    for j in range(4):
        for i in range(4):
            sp = lax.rem(pos[0] + steps[i] + 4, 4) * 4 + lax.rem(pos[1] + steps[j] + 4, 4)
            at = pl.ds(pl.multiple_of(sp * 128, 128), 128)
            src, off = ((parts[0], 0), (parts[1], 0), (parts[2], 0), (parts[2], 512))[j]
            cols = slice(off + i * 128, off + (i + 1) * 128)
            total = src[0][:, cols].astype(f32) + src[1][:, cols].astype(f32)
            total = total + src[2][:, cols].astype(f32) + src[3][:, cols].astype(f32)
            out_ref[:, at] = (res_ref[:, at].astype(f32) + total).astype(bf16)


def relay_kernel(*refs):
    out_ref, held, sems = refs[4:]
    inward = [pltpu.make_async_copy(refs[i], held.at[i], sems.at[i]) for i in range(4)]
    outward = [pltpu.make_async_copy(held.at[i], out_ref.at[i], sems.at[4 + i]) for i in range(4)]
    for copy in inward:
        copy.start()
    for i in range(4):
        inward[i].wait()
        outward[i].start()
    for copy in outward:
        copy.wait()


def join_kernel(*refs):
    out_ref, sems = refs[4:]
    copies = [pltpu.make_async_copy(refs[i], out_ref.at[i], sems.at[i]) for i in range(4)]
    for copy in copies:
        copy.start()
    for copy in copies:
        copy.wait()


def load_kernel(w_ref, out_ref, sem):
    copy = pltpu.make_async_copy(w_ref, out_ref, sem)
    copy.start()
    copy.wait()


def call(kernel, ins, outs, scratch, args, flops, nbytes, limit, spec=VMEM):
    return launched(kernel, ins, outs, scratch, args, flops, nbytes, limit, spec)


def launched(kernel, ins, outs, scratch, args, flops, nbytes, limit, spec):
    return pl.pallas_call(
        kernel,
        in_specs=ins,
        out_specs=[spec] * len(outs),
        out_shape=[jax.ShapeDtypeStruct(s, t) for s, t in outs],
        scratch_shapes=scratch,
        cost_estimate=pl.CostEstimate(flops=flops, bytes_accessed=nbytes, transcendentals=0),
        compiler_params=pltpu.CompilerParams(vmem_limit_bytes=limit * 1024 * 1024),
    )(*args)


def shifted(v, axis, by, n=4):
    return lax.ppermute(v, axis, [(i, (i + by) % n) for i in range(n)])


def swapped(v):
    return lax.ppermute(v, "c", [(0, 1), (1, 0)])


def both_ways(v, axis, sign):
    pairs = [(2 * i + c, 2 * ((i + sign * (1 - 2 * c)) % 4) + c) for i in range(4) for c in range(2)]
    return lax.ppermute(v, (axis, "c"), pairs)


def relayed(blocks):
    shape = (4, *blocks[0].shape)
    scratch = [pltpu.VMEM(shape, bf16), pltpu.SemaphoreType.DMA((8,))]
    return call(relay_kernel, [HBM] * 4, [(shape, bf16)], scratch, blocks, 800_000_000, 2_000_000, 60, HBM)[0]


def joined(blocks):
    shape = (4, *blocks[0].shape)
    scratch = [pltpu.SemaphoreType.DMA((4,))]
    return call(join_kernel, [VMEM] * 4, [(shape, bf16)], scratch, blocks, 800_000_000, 2_000_000, 4, HBM)[0]


def local(
    queries,
    keys,
    values,
    out_gate,
    decay_logit,
    head_gain,
    out_weight,
    stream,
    mlp_gain,
    up_weight,
    down_weight,
):
    length = queries.shape[0]

    up_a, up_b = both_ways(up_weight, "y", 1), both_ways(up_weight, "y", -1)
    down_a, down_b = both_ways(down_weight, "z", 1), both_ways(down_weight, "z", -1)

    rows_out, carry, sent = call(
        attend_kernel,
        [VMEM] * 4,
        [((length, HEAD_V), f32), ((length, 2 * HEAD_K), bf16), ((PEERS, FOLD, 128), bf16)],
        [
            pltpu.VMEM((length, 2 * HEAD_K), f32),
            pltpu.VMEM((length // BLOCK, 2 * HEAD_K), f32),
            pltpu.VMEM((length // BLOCK, HEAD_V, 2 * HEAD_K), f32),
        ],
        (queries.T, keys.T, values, decay_logit.transpose(0, 2, 1)),
        2_000_000_000,
        2_000_000,
        60,
    )
    up_2 = both_ways(up_a, "y", 1)
    down_2 = both_ways(down_a, "z", 1)
    streams = [stream] + [shifted(stream, "x", NEAR[k]) for k in (3, 2, 1)]
    streams = [streams[0], streams[2], streams[3], streams[1]]
    got = lax.all_to_all(sent, SP, 0, 0, tiled=True)
    up_line = joined((up_weight, up_a, up_b, up_2))
    down_line = relayed((down_weight, down_a, down_b, down_2))
    up_na, up_nb = both_ways(up_line, "z", 1), both_ways(up_line, "z", -1)
    down_na, down_nb = both_ways(down_line, "y", 1), both_ways(down_line, "y", -1)
    up_n2 = both_ways(up_na, "z", 1)
    down_n2 = both_ways(down_na, "y", 1)
    ups = [up_line, up_na, up_nb, up_n2]
    ups_s = [swapped(v) for v in ups]
    downs = [down_line, down_na, down_nb, down_n2]
    downs_s = [swapped(v) for v in downs]
    keep, give = call(
        gate_kernel,
        [VMEM, HBM, HBM, HBM, VMEM],
        [((4, ROWS, HEAD_V), bf16)] * 2,
        [
            pltpu.VMEM((2, 4, ROWS, HEAD_V), bf16),
            pltpu.VMEM((length, HEAD_V), f32),
            pltpu.VMEM((length, 2 * HEAD_K), bf16),
            pltpu.VMEM((length, HEAD_V), bf16),
            pltpu.SemaphoreType.DMA((3,)),
        ],
        (got, rows_out, carry, out_gate, head_gain.reshape(1, HEAD_V)),
        1_000_000_000,
        2_000_000,
        60,
    )
    pair = jnp.stack([keep, swapped(give)])
    heads = {k: shifted(pair, "x", NEAR[k]) for k in (1, 2, 3)}
    heads = [pair, heads[2], heads[1], heads[3]]
    mixing = call(
        load_kernel,
        [HBM],
        [(out_weight.shape, bf16)],
        [pltpu.SemaphoreType.DMA],
        (out_weight,),
        1000,
        10000,
        1,
    )[0]
    near, far, residual = call(
        mix_kernel,
        [VMEM] * 10,
        [((4 * ROWS, 1536), bf16), ((4 * ROWS, 512), bf16), ((ROWS, D), bf16)],
        [
            pltpu.VMEM((4 * ROWS, 1024), bf16),
            pltpu.VMEM((4 * ROWS, D), bf16),
        ],
        (*heads, *streams, mixing, mlp_gain.reshape(1, D)),
        2 * 512 * 1024 * 2048,
        12_000_000,
        24,
    )
    gathered = call(
        up_kernel,
        [VMEM] + [ANY] * 6,
        [((4 * ROWS, 2048), f32)],
        [pltpu.VMEM((1536, 2048), bf16), pltpu.SemaphoreType.DMA((24,))],
        (near, *[w for j in range(3) for w in (ups[j], ups_s[TURNED[j]])]),
        2 * 512 * 1536 * 2048,
        10_000_000,
        20,
    )[0]
    turned = call(
        turn_kernel,
        [VMEM] * 2 + [ANY] * 4,
        [((4 * ROWS, 2048), bf16)] + [((ROWS, 512), bf16)] * 4,
        [pltpu.VMEM((512, 2048), bf16), pltpu.VMEM((2048, 512), bf16), pltpu.SemaphoreType.DMA((16,))],
        (far, gathered, ups[3], ups_s[3], downs[0], downs_s[0]),
        4 * 512 * 512 * 2048,
        8_000_000,
        24,
    )
    hidden, first = turned[0], turned[1:]

    def down(js):
        count = len(js)
        return call(
            functools.partial(down_kernel, count=count),
            [VMEM] + [ANY] * (2 * count),
            [((ROWS, count * 512), bf16)] * 4,
            [pltpu.VMEM((2048, count * 512), bf16), pltpu.SemaphoreType.DMA((8 * count,))],
            (hidden, *[w for j in js for w in (downs[j], downs_s[TURNED[j]])]),
            count * 512 * 2048 * 1024,
            count * 3_000_000,
            20,
        )

    def sent_back(parts):
        return [parts[0]] + [shifted(parts[k], "x", NEAR[k]) for k in (1, 2, 3)]

    first = sent_back(first)
    second = sent_back(down((1,)))
    third = sent_back(down((2, 3)))
    return call(
        end_kernel,
        [VMEM] * 13,
        [((ROWS, D), bf16)],
        [],
        (residual, *first, *second, *third),
        100_000_000,
        3_000_000,
        8,
    )[0]


def solution(mesh):
    split = Mesh(mesh.devices.reshape(4, 4, 4, 2), ("z", "y", "x", "c"))
    both = SP + TP
    in_specs = (
        P(SP, TP),
        P(SP, TP),
        P(SP, TP),
        P(SP, TP),
        P(None, SP, TP),
        P(TP),
        P(),
        P(both, None),
        P(),
        P(SP, TP),
        P(TP, SP),
    )
    return jax.shard_map(local, mesh=split, in_specs=in_specs, out_specs=P(both, None), check_vma=False)
```
